32 devices in a mesh: sp: 16 (over z, y, x), tp: 2 (over core).
Axes of the slice: x: 2, y: 2, z: 4, core: 2. Of those that a mesh axis runs over, the one named last changes fastest.
Arguments:
- x_rows: bfloat16 [2048, 2048], P('sp'), may hold values from -6 to 6
- queries: bfloat16 [2048, 1024], P('sp', 'tp'), may hold values from -8 to 8
- keys: bfloat16 [2048, 512], P('sp', 'tp'), may hold values from -8 to 8
- values: bfloat16 [2048, 512], P('sp', 'tp'), may hold values from -6 to 6
- query_norm_gain: float32 [64], replicated, may hold values from 1 to 8
- key_norm_gain: float32 [64], replicated, may hold values from 1 to 8
- out_weight: bfloat16 [1024, 2048], P('tp'), may hold values from -0.1875 to 0.1875
- ffn_gain: float32 [2048], replicated, may hold values from 0.1 to 1.9
- gate_weight: bfloat16 [2048, 5120], P('sp', 'tp'), may hold values from -0.125 to 0.125
- value_weight: bfloat16 [2048, 5120], P('sp', 'tp'), may hold values from -0.125 to 0.125
- conv_gate: float32 [3, 5120], P(None, 'tp'), may hold values from -3.5 to 3.5
- conv_value: float32 [3, 5120], P(None, 'tp'), may hold values from -3.5 to 3.5
- down_weight: bfloat16 [2048, 5120], P('sp', 'tp'), may hold values from -0.078125 to 0.078125
Outputs:
- layer_out: bfloat16 [2048, 2048], P('sp')
The draws below stay inside these ranges and needn't reach their ends.
All inputs are finite; a program needn't handle non-finite values.
Results may differ from the reference program's by a relative error of at most 0.017.
Values may be sent and summed in bfloat16 or wider, within the bound.
A program may use at most 64 MiB of HBM per device.

```python
import math
import jax
import jax.numpy as jnp
from jax import lax

D = 2048
QUERY_HEAD_COUNT = 16
KEY_VALUE_HEADS = 8
HEAD_SIZE = 64
FF = 5120
GRID_ROW_WIDTH = 64
TOKEN_TOTAL = 2048
N_TP = 2


def gain_draw(key, salt_value):
    sub_key = jax.random.fold_in(key, salt_value)
    return jax.random.uniform(sub_key, (HEAD_SIZE,), jnp.float32, 1.0, 2.2)


def draw_query_norm_gain(key, part):
    return gain_draw(key, 101)


def draw_key_norm_gain(key, part):
    return gain_draw(key, 202)


def draw_queries(key, part):
    baseline_rows = jnp.clip(jax.random.normal(jax.random.fold_in(key, 505), (TOKEN_TOTAL, QUERY_HEAD_COUNT, HEAD_SIZE), jnp.float32), -6.0, 6.0)
    return jnp.clip(baseline_rows, -8.0, 8.0).reshape(TOKEN_TOTAL, QUERY_HEAD_COUNT * HEAD_SIZE).astype(jnp.bfloat16)


def draw_keys(key, part):
    baseline_rows = jnp.clip(jax.random.normal(jax.random.fold_in(key, 606), (TOKEN_TOTAL, KEY_VALUE_HEADS, HEAD_SIZE), jnp.float32), -6.0, 6.0)
    return jnp.clip(baseline_rows, -8.0, 8.0).reshape(TOKEN_TOTAL, KEY_VALUE_HEADS * HEAD_SIZE).astype(jnp.bfloat16)


def shard_levels(key, shape, shards, smallest, top_value):
    def one(axis_at, blocks):
        draws = jax.random.uniform(jax.random.fold_in(jax.random.fold_in(key, 6), axis_at), (blocks,), jnp.float32, smallest / len(shards), top_value / len(shards))
        return jnp.repeat(jnp.exp(draws), shape[axis_at] // blocks).reshape((-1,) + (1,) * (len(shape) - axis_at - 1))

    factor_of = one(*shards[0])
    for cut in shards[1:]:
        factor_of = factor_of * one(*cut)
    return factor_of


def scatter_about(key, extent, deviation, bound, shards=(), kind=jnp.bfloat16):
    values = jax.random.normal(key, extent, jnp.float32) * deviation
    if len(shards) > 0:
        values = shard_levels(key, extent, shards, -0.22, 0.18) * values
    return jnp.clip(values, min=-bound, max=bound).astype(kind)


def setup_inputs(seed: int = 0) -> dict:
    seeds = jax.random.split(jax.random.key(seed), 14)
    x_rows = scatter_about(seeds[0], (TOKEN_TOTAL, D), 1.0, 6.0, ((0, 16),))
    queries = draw_queries(jax.random.fold_in(seeds[13], 71), 0)
    keys = draw_keys(jax.random.fold_in(seeds[13], 71), 0)
    values = scatter_about(seeds[3], (TOKEN_TOTAL, KEY_VALUE_HEADS * HEAD_SIZE), 1.0, 6.0, ((0, 16), (1, 2)))
    query_norm_gain = draw_query_norm_gain(jax.random.fold_in(seeds[13], 71), 0)
    key_norm_gain = draw_key_norm_gain(jax.random.fold_in(seeds[13], 71), 0)
    out_weight = scatter_about(seeds[6], (QUERY_HEAD_COUNT * HEAD_SIZE, D), (QUERY_HEAD_COUNT * HEAD_SIZE) ** -0.5, 0.1875, ((0, 2),))
    ffn_gain = jnp.clip(1.0 + 0.18 * jax.random.normal(seeds[7], (D,), jnp.float32), 0.1, 1.9)
    gate_weight = scatter_about(seeds[8], (D, FF), D ** -0.5, 0.125, ((0, 16), (1, 2)))
    value_weight = scatter_about(seeds[9], (D, FF), D ** -0.5, 0.125, ((0, 16), (1, 2)))
    conv_gate = scatter_about(seeds[10], (3, FF), 3 ** -0.5, 3.5, ((1, 2),), jnp.float32)
    conv_value = scatter_about(seeds[11], (3, FF), 3 ** -0.5, 3.5, ((1, 2),), jnp.float32)
    down_weight = scatter_about(seeds[12], (D, FF), FF ** -0.5, 0.078125, ((0, 16), (1, 2)))
    return dict(x_rows=x_rows, queries=queries, keys=keys, values=values, query_norm_gain=query_norm_gain, key_norm_gain=key_norm_gain, out_weight=out_weight, ffn_gain=ffn_gain, gate_weight=gate_weight, value_weight=value_weight, conv_gate=conv_gate, conv_value=conv_value, down_weight=down_weight)


eps_norm = 1e-06
theta = 10000.0

def per_head_norm(head_block, gain_vec):
    wide_vals = head_block.astype(jnp.float32)
    inverse_rms = lax.rsqrt(lax.optimization_barrier(jnp.mean(wide_vals * wide_vals, axis=-1, keepdims=True)) + eps_norm)
    return wide_vals * inverse_rms * gain_vec

def turn_half(half_vec, places):
    quarter_len = half_vec.shape[-1] // 2
    inverse_rates = 1.0 / theta ** (jnp.arange(quarter_len, dtype=jnp.float32) * 2.0 / half_vec.shape[-1])
    angles = places.astype(jnp.float32)[:, None] * inverse_rates[None, :]
    angles = jnp.concatenate([angles, angles], axis=-1)[:, None, :]
    front_part = half_vec[..., :quarter_len]
    back_part = half_vec[..., quarter_len:]
    return half_vec * jnp.cos(angles) + jnp.concatenate([-back_part, front_part], axis=-1) * jnp.sin(angles)

def apply_rotary(normed_heads, token_positions):
    half_point = normed_heads.shape[-1] // 2
    grid_row = token_positions // GRID_ROW_WIDTH
    grid_col = token_positions % GRID_ROW_WIDTH
    return jnp.concatenate([turn_half(normed_heads[..., :half_point], grid_row), turn_half(normed_heads[..., half_point:], grid_col)], axis=-1)

def row_norm(rows_wide, gain_vec):
    inverse_rms = lax.rsqrt(lax.optimization_barrier(jnp.mean(rows_wide * rows_wide, axis=-1, keepdims=True)) + eps_norm)
    return (rows_wide * inverse_rms * gain_vec).astype(jnp.bfloat16)

def conv_rows(pre_rows, conv_taps):
    padded = jnp.pad(pre_rows.astype(jnp.float32), ((1, 1), (0, 0)))
    return conv_taps[0] * padded[:-2] + conv_taps[1] * padded[1:-1] + conv_taps[2] * padded[2:]

def reference(x_rows, queries, keys, values, query_norm_gain, key_norm_gain, out_weight, ffn_gain, gate_weight, value_weight, conv_gate, conv_value, down_weight):
    token_number = x_rows.shape[0]
    token_positions = jnp.arange(token_number, dtype=jnp.int32)
    group_width = QUERY_HEAD_COUNT // KEY_VALUE_HEADS
    rotated_queries = apply_rotary(per_head_norm(queries.reshape(token_number, QUERY_HEAD_COUNT, HEAD_SIZE), query_norm_gain), token_positions).reshape(token_number, KEY_VALUE_HEADS, group_width, HEAD_SIZE)
    rotated_keys = apply_rotary(per_head_norm(keys.reshape(token_number, KEY_VALUE_HEADS, HEAD_SIZE), key_norm_gain), token_positions)
    value_matrix = values.reshape(token_number, KEY_VALUE_HEADS, HEAD_SIZE).astype(jnp.float32)
    query_span = math.gcd(token_number, 128)
    block_starts = jnp.arange(token_number // query_span, dtype=jnp.int32) * query_span

    def attend_block(first_row):
        query_block = lax.dynamic_slice_in_dim(rotated_queries, first_row, query_span, 0)
        scores = jnp.einsum('qkgd,skd->kgqs', query_block, rotated_keys, precision=lax.Precision.HIGHEST) * HEAD_SIZE ** (-0.5)
        shifted = jnp.exp(scores - lax.optimization_barrier(jnp.max(scores, axis=-1, keepdims=True)))
        denominator = lax.optimization_barrier(jnp.sum(shifted, axis=-1))
        weights = lax.optimization_barrier(shifted.astype(jnp.bfloat16)).astype(jnp.float32)
        summed = jnp.einsum('kgqs,skd->qkgd', weights, value_matrix, precision=lax.Precision.HIGHEST)
        return (summed / jnp.transpose(denominator, (2, 0, 1))[..., None]).astype(jnp.bfloat16)
    attended_blocks = lax.map(attend_block, block_starts)
    attended = attended_blocks.reshape(token_number, QUERY_HEAD_COUNT * HEAD_SIZE)
    head_width = QUERY_HEAD_COUNT * HEAD_SIZE // N_TP

    def head_part(running, group_index):
        part = jnp.dot(lax.dynamic_slice_in_dim(attended, group_index * head_width, head_width, 1), lax.dynamic_slice_in_dim(out_weight, group_index * head_width, head_width, 0), preferred_element_type=jnp.float32)
        return (running + lax.optimization_barrier(part.astype(jnp.bfloat16)).astype(jnp.float32), None)
    head_branch, _ = lax.scan(head_part, jnp.zeros((token_number, D), jnp.float32), jnp.arange(N_TP, dtype=jnp.int32))
    middle_rows = x_rows.astype(jnp.float32) + head_branch
    normed = row_norm(middle_rows, ffn_gain)
    gate_pre = jnp.dot(normed, gate_weight, preferred_element_type=jnp.float32).astype(jnp.bfloat16)
    value_pre = jnp.dot(normed, value_weight, preferred_element_type=jnp.float32).astype(jnp.bfloat16)
    hidden = (jax.nn.silu(conv_rows(gate_pre, conv_gate)) * conv_rows(value_pre, conv_value)).astype(jnp.bfloat16)
    unit_width = FF // N_TP

    def unit_part(running, group_index):
        part = lax.dot_general(lax.dynamic_slice_in_dim(hidden, group_index * unit_width, unit_width, 1), lax.dynamic_slice_in_dim(down_weight, group_index * unit_width, unit_width, 1), (((1,), (1,)), ((), ())), preferred_element_type=jnp.float32)
        return (running + lax.optimization_barrier(part.astype(jnp.bfloat16)).astype(jnp.float32), None)
    unit_branch, _ = lax.scan(unit_part, jnp.zeros((token_number, D), jnp.float32), jnp.arange(N_TP, dtype=jnp.int32))
    return (middle_rows + unit_branch).astype(jnp.bfloat16)
```

```python
import functools
import math

import jax
import jax.numpy as jnp
from jax import lax
from jax.experimental import pallas as pl
from jax.experimental.pallas import tpu as pltpu
from jax.sharding import PartitionSpec as P

HEAD_SIZE = 64
GRID_ROW_WIDTH = 64


eps_norm = 1e-06
theta = 10000.0


def with_halo(cells, sides, width):
    for axis, dim in sides:
        count = lax.axis_size(axis)
        ends = count - 1
        head = lax.slice_in_dim(cells, 0, width, axis=dim)
        tail = lax.slice_in_dim(cells, cells.shape[dim] - width, cells.shape[dim], axis=dim)
        cells = jnp.concatenate(
            [
                lax.ppermute(tail, axis, [(i, (i + 1) % count) for i in range(ends)]),
                cells,
                lax.ppermute(head, axis, [((i + 1) % count, i) for i in range(ends)]),
            ],
            axis=dim,
        )
    return cells


def per_head_norm(head_block, gain_vec):
    wide_vals = head_block.astype(jnp.float32)
    inverse_rms = lax.rsqrt(jnp.mean(wide_vals * wide_vals, axis=-1, keepdims=True) + eps_norm)
    return wide_vals * inverse_rms * gain_vec


def turn_half(half_vec, places):
    quarter_len = half_vec.shape[-1] // 2
    inverse_rates = 1.0 / theta ** (
        jnp.arange(quarter_len, dtype=jnp.float32) * 2.0 / half_vec.shape[-1]
    )
    angles = places.astype(jnp.float32)[:, None] * inverse_rates[None, :]
    angles = jnp.concatenate([angles, angles], axis=-1)[:, None, :]
    front_part = half_vec[..., :quarter_len]
    back_part = half_vec[..., quarter_len:]
    return half_vec * jnp.cos(angles) + jnp.concatenate(
        [-back_part, front_part], axis=-1
    ) * jnp.sin(angles)


def apply_rotary(normed_heads, token_positions):
    half_point = normed_heads.shape[-1] // 2
    grid_row = token_positions // GRID_ROW_WIDTH
    grid_col = token_positions % GRID_ROW_WIDTH
    return jnp.concatenate(
        [
            turn_half(normed_heads[..., :half_point], grid_row),
            turn_half(normed_heads[..., half_point:], grid_col),
        ],
        axis=-1,
    )


def row_norm(rows_wide, gain_vec):
    inverse_rms = lax.rsqrt(jnp.mean(rows_wide * rows_wide, axis=-1, keepdims=True) + eps_norm)
    return (rows_wide * inverse_rms * gain_vec).astype(jnp.bfloat16)


def contract_units(left_rows, right_rows):
    return lax.dot_general(
        left_rows, right_rows, (((1,), (1,)), ((), ())), preferred_element_type=jnp.float32
    )


def shards(
    x_rows,
    queries,
    keys,
    values,
    query_norm_gain,
    key_norm_gain,
    out_weight,
    ffn_gain,
    gate_weight,
    value_weight,
    conv_gate,
    conv_value,
    down_weight,
):
    collected = (
        lax.all_gather(gate_weight, "sp", axis=0, tiled=True),
        lax.all_gather(value_weight, "sp", axis=0, tiled=True),
        lax.all_gather(down_weight, "sp", axis=0, tiled=True),
    )
    tokens_here = queries.shape[0]
    query_heads = queries.shape[1] // HEAD_SIZE
    key_heads = keys.shape[1] // HEAD_SIZE
    group_width = query_heads // key_heads
    lane_rows = group_width * tokens_here
    token_positions = lax.axis_index("sp") * tokens_here + jnp.arange(tokens_here, dtype=jnp.int32)
    rotated_queries = apply_rotary(
        per_head_norm(queries.reshape(tokens_here, query_heads, HEAD_SIZE), query_norm_gain),
        token_positions,
    )
    query_lanes = rotated_queries.reshape(tokens_here, key_heads, group_width, HEAD_SIZE).transpose(
        1, 2, 0, 3
    )
    query_lanes = query_lanes.reshape(key_heads, lane_rows, HEAD_SIZE) * HEAD_SIZE ** (-0.5)
    start_state = (
        jnp.full((key_heads, lane_rows), -1e30, jnp.float32),
        jnp.zeros((key_heads, lane_rows), jnp.float32),
        jnp.zeros((key_heads, lane_rows, HEAD_SIZE), jnp.float32),
    )
    key_piece = lax.all_gather(keys, "sp", axis=0, tiled=True)
    value_piece = lax.all_gather(values, "sp", axis=0, tiled=True)
    row_count = key_piece.shape[0]
    key_places = jnp.arange(row_count, dtype=jnp.int32)
    turned = apply_rotary(
        per_head_norm(key_piece.reshape(row_count, key_heads, HEAD_SIZE), key_norm_gain), key_places
    )
    key_span = math.gcd(row_count, 2048)
    span_count = row_count // key_span
    turned = turned.reshape(span_count, key_span, key_heads, HEAD_SIZE)
    value_matrix = value_piece.reshape(span_count, key_span, key_heads, HEAD_SIZE)

    def one_span(state_now, inputs):
        running_top, denominator, weighted = state_now
        key_block, value_block = inputs
        scores = jnp.einsum("hrd,shd->hrs", query_lanes, key_block, precision=lax.Precision.HIGHEST)
        new_top = jnp.maximum(running_top, jnp.max(scores, axis=-1))
        factor = jnp.exp(running_top - new_top)
        weights = jnp.exp(scores - new_top[..., None])
        denominator = denominator * factor + jnp.sum(weights, axis=-1)
        weighted = weighted * factor[..., None] + jnp.einsum(
            "hrs,shd->hrd",
            weights.astype(jnp.bfloat16),
            value_block,
            preferred_element_type=jnp.float32,
        )
        return ((new_top, denominator, weighted), None)

    folded_state, _ = lax.scan(one_span, start_state, (turned, value_matrix))
    running_top, denominator, weighted = folded_state
    attended = (weighted / denominator[..., None]).reshape(
        key_heads, group_width, tokens_here, HEAD_SIZE
    )
    attended = (
        attended.transpose(2, 0, 1, 3)
        .reshape(tokens_here, query_heads * HEAD_SIZE)
        .astype(jnp.bfloat16)
    )
    share_rows = tokens_here // lax.axis_size("tp")
    head_share = lax.psum_scatter(
        jnp.dot(attended, out_weight, preferred_element_type=jnp.float32).astype(jnp.bfloat16),
        "tp",
        scatter_dimension=0,
        tiled=True,
    ).astype(jnp.float32)
    own_rows = lax.dynamic_slice_in_dim(x_rows, lax.axis_index("tp") * share_rows, share_rows, 0)
    middle_rows = own_rows.astype(jnp.float32) + head_share
    normed = lax.all_gather(row_norm(middle_rows, ffn_gain), "tp", axis=0, tiled=True)
    unit_local = gate_weight.shape[1]
    gate_pre = jnp.dot(normed, collected[0], preferred_element_type=jnp.float32).astype(
        jnp.bfloat16
    )
    value_pre = jnp.dot(normed, collected[1], preferred_element_type=jnp.float32).astype(
        jnp.bfloat16
    )
    joined = jnp.concatenate([gate_pre, value_pre], axis=1)
    padded = with_halo(joined, (("sp", 0),), 1).astype(jnp.float32)
    conv_taps = jnp.concatenate([conv_gate, conv_value], axis=1)
    convolved = conv_taps[0] * padded[:-2] + conv_taps[1] * padded[1:-1] + conv_taps[2] * padded[2:]
    hidden = (jax.nn.silu(convolved[:, :unit_local]) * convolved[:, unit_local:]).astype(
        jnp.bfloat16
    )
    unit_share = lax.psum_scatter(
        contract_units(hidden, collected[2]).astype(jnp.bfloat16),
        "tp",
        scatter_dimension=0,
        tiled=True,
    ).astype(jnp.float32)
    finished = (middle_rows + unit_share).astype(jnp.bfloat16)
    return lax.all_gather(finished, "tp", axis=0, tiled=True)

LANES = 128
MESH = pl.DeviceIdType.MESH
BF = jnp.bfloat16
F32 = jnp.float32


def nt(left, right):
    return lax.dot_general(left, right, (((1,), (1,)), ((), ())), preferred_element_type=F32)


def layer_kernel(
    n, halves, x_ref, q_ref, kv_ref, qg_ref, kg_ref, cos_ref, sin_ref, wo_ref, fg_ref, w_ref,
    cg_ref, cv_ref, out_ref,
    kvbuf, qbuf, kcat, qcat, att_s, attbuf, po_s, po_r, mid, allnorm, halo_s, halo_r, wrecv,
    pre_g, pre_v, part, ddbuf, own_sum, rs_s, rs_r, fin_s, fin_r,
    loc, kv_ss, kv_rs, q_ss, q_rs, w_ss, w_rs, o_ss, o_rs, po_sem, ag_ss, ag_rs, fw_ss, fw_rs,
    h_ss, h_rs, dd_ss, dd_rs, c_ss, c_rs, fin_sem,
):
    sp = lax.axis_index("sp")
    core = lax.axis_index("tp")
    mate = 1 - core
    rows = x_ref.shape[0]
    half_rows = rows // 2
    width = x_ref.shape[1]
    kv_heads = kv_ref.shape[1] // LANES
    group = n // halves
    tokens = n * rows
    q_tokens = kv_heads * rows
    units = w_ref.shape[1] // 3
    head_at = lax.rem(sp, kv_heads)
    q_base = sp - head_at
    in_group = lax.rem(sp, group)
    g_base = sp - in_group
    half_at = sp // group

    def remote(src, dst, ss, rs, device):
        return pltpu.make_async_remote_copy(
            src_ref=src, dst_ref=dst, send_sem=ss, recv_sem=rs, device_id=device, device_id_type=MESH
        )

    def lane_block(k):
        return pl.ds(pl.multiple_of(k * LANES, LANES), LANES)

    def span(start, size, unit):
        return pl.ds(pl.multiple_of(start, unit), size)

    def loop(lo, hi, fn):
        def step(k, carry):
            fn(k)
            return carry

        lax.fori_loop(lo, hi, step, 0)

    barrier = pltpu.get_barrier_semaphore()

    def greet(d):
        t = lax.rem(sp + d, n)
        pl.semaphore_signal(barrier, inc=1, device_id=(t, core), device_id_type=MESH)
        pl.semaphore_signal(barrier, inc=1, device_id=(t, mate), device_id_type=MESH)

    loop(1, n, greet)
    pl.semaphore_signal(barrier, inc=1, device_id=(sp, mate), device_id_type=MESH)
    pl.semaphore_wait(barrier, 2 * n - 1)

    def q_copy(d):
        t = q_base + lax.rem(head_at + d, kv_heads)
        return remote(
            q_ref.at[:, lane_block(t - q_base)], qbuf.at[span(head_at * rows, rows, rows)],
            q_ss.at[d], q_rs.at[d], (t, core),
        )

    def kv_copy(d):
        t = lax.rem(sp + d, n)
        return remote(
            kv_ref.at[:, lane_block(lax.rem(t, kv_heads))], kvbuf.at[span(sp * rows, rows, rows)],
            kv_ss.at[d], kv_rs.at[d], (t, core),
        )

    def w_copy(d):
        t = lax.rem(sp + d, n)
        return remote(
            w_ref.at[lax.rem(t, group)], wrecv.at[:, lane_block(sp)],
            w_ss.at[d], w_rs.at[d], (t, core),
        )

    own_q = pltpu.make_async_copy(
        q_ref.at[:, lane_block(head_at)], qbuf.at[span(head_at * rows, rows, rows)], loc.at[0]
    )
    own_kv = pltpu.make_async_copy(
        kv_ref.at[:, lane_block(head_at)], kvbuf.at[span(sp * rows, rows, rows)], loc.at[1]
    )
    own_w = pltpu.make_async_copy(w_ref.at[in_group], wrecv.at[:, lane_block(sp)], loc.at[2])
    own_q.start()
    own_kv.start()
    loop(1, kv_heads, lambda d: q_copy(d).start())
    loop(1, n, lambda d: kv_copy(d).start())
    loop(1, n, lambda d: w_copy(d).start())
    own_w.start()

    lane = lax.broadcasted_iota(jnp.int32, (GRID_ROW_WIDTH, LANES), 1)
    low = lane < HEAD_SIZE
    first = lax.rem(lane, 2 * HEAD_SIZE // 4) < HEAD_SIZE // 4
    by_row = lax.rem(lane, HEAD_SIZE) < HEAD_SIZE // 2

    def turn(vals, grid_row):
        cos = jnp.where(by_row, cos_ref[pl.ds(grid_row, 1), :], cos_ref[:GRID_ROW_WIDTH, :])
        sin = jnp.where(by_row, sin_ref[pl.ds(grid_row, 1), :], sin_ref[:GRID_ROW_WIDTH, :])
        quarter = HEAD_SIZE // 4
        swapped = jnp.where(
            first, pltpu.roll(vals, LANES - quarter, 1), pltpu.roll(vals, quarter, 1)
        )
        return vals * cos + swapped * sin

    def split(vals):
        top = vals.astype(BF).astype(F32)
        return top, (vals - top).astype(BF).astype(F32)

    own_q.wait()

    def q_wait(d):
        s = lax.rem(head_at + kv_heads - d, kv_heads)
        dst = qbuf.at[span(s * rows, rows, rows)]
        remote(dst, dst, q_ss.at[d], q_rs.at[d], (q_base + s, core)).wait_recv()

    loop(1, kv_heads, q_wait)

    def make_q(r):
        at = span(r * GRID_ROW_WIDTH, GRID_ROW_WIDTH, GRID_ROW_WIDTH)
        vals = qbuf[at, :].astype(F32)
        sq = vals * vals
        low_sum = jnp.sum(jnp.where(low, sq, 0.0), axis=1, keepdims=True)
        high_sum = jnp.sum(jnp.where(low, 0.0, sq), axis=1, keepdims=True)
        inverse = jnp.where(
            low,
            lax.rsqrt(low_sum * (1.0 / HEAD_SIZE) + eps_norm),
            lax.rsqrt(high_sum * (1.0 / HEAD_SIZE) + eps_norm),
        )
        turned = turn(vals * inverse * qg_ref[...], q_base * (rows // GRID_ROW_WIDTH) + r)
        top, rest = split(turned * HEAD_SIZE ** (-0.5))
        qcat[at, :] = jnp.where(low, top, pltpu.roll(rest, HEAD_SIZE, 1)).astype(BF)
        later = span(q_tokens + r * GRID_ROW_WIDTH, GRID_ROW_WIDTH, GRID_ROW_WIDTH)
        qcat[later, :] = jnp.where(low, pltpu.roll(top, HEAD_SIZE, 1), rest).astype(BF)

    loop(0, q_tokens // GRID_ROW_WIDTH, make_q)
    own_kv.wait()

    def kv_wait(d):
        s = lax.rem(sp + n - d, n)
        dst = kvbuf.at[span(s * rows, rows, rows)]
        remote(dst, dst, kv_ss.at[d], kv_rs.at[d], (s, core)).wait_recv()

    loop(1, n, kv_wait)

    def make_k(r):
        at = span(r * GRID_ROW_WIDTH, GRID_ROW_WIDTH, GRID_ROW_WIDTH)
        vals = kvbuf[at, :].astype(F32)
        total = jnp.sum(jnp.where(low, vals * vals, 0.0), axis=1, keepdims=True)
        turned = turn(
            vals * lax.rsqrt(total * (1.0 / HEAD_SIZE) + eps_norm) * kg_ref[...], r
        )
        top, rest = split(turned)
        kcat[at, :LANES] = jnp.where(low, top, pltpu.roll(top, HEAD_SIZE, 1)).astype(BF)
        kcat[at, LANES:] = jnp.where(low, rest, pltpu.roll(rest, HEAD_SIZE, 1)).astype(BF)

    loop(0, tokens // GRID_ROW_WIDTH, make_k)

    def o_copy(d):
        k = lax.rem(head_at + d, kv_heads)
        return remote(
            att_s.at[span(k * rows, rows, rows)], attbuf.at[:, lane_block(head_at)],
            o_ss.at[d], o_rs.at[d], (q_base + k, core),
        )

    low_rows = lax.broadcasted_iota(jnp.int32, (rows, LANES), 1) < HEAD_SIZE

    def attend(k):
        both = jnp.concatenate(
            [qcat[span(k * rows, rows, rows), :], qcat[span(q_tokens + k * rows, rows, rows), :]],
            axis=0,
        )
        scores = nt(jnp.concatenate([both, both], axis=1), kcat[...])
        shifted = jnp.exp(scores - jnp.max(scores, axis=1, keepdims=True))
        total = jnp.sum(shifted, axis=1, keepdims=True)
        summed = jnp.dot(shifted.astype(BF), kvbuf[...], preferred_element_type=F32) / total
        return jnp.where(
            low_rows, pltpu.roll(summed[:rows], HEAD_SIZE, 1), summed[rows:]
        ).astype(BF)

    def attend_send(d):
        k = lax.rem(head_at + d, kv_heads)
        att_s[span(k * rows, rows, rows), :] = attend(k)

        @pl.when(d < kv_heads)
        def _():
            o_copy(d).start()

    loop(1, kv_heads + 1, attend_send)
    attbuf[:, lane_block(head_at)] = att_s[span(head_at * rows, rows, rows), :]

    def o_wait(d):
        s = lax.rem(head_at + kv_heads - d, kv_heads)
        dst = attbuf.at[:, lane_block(s)]
        remote(dst, dst, o_ss.at[d], o_rs.at[d], (q_base + s, core)).wait_recv()

    loop(1, kv_heads, o_wait)

    po_s[...] = jnp.dot(attbuf[...], wo_ref[...], preferred_element_type=F32).astype(BF)
    po_copy = remote(
        po_s.at[span(mate * half_rows, half_rows, half_rows)], po_r, po_sem.at[0], po_sem.at[1],
        (sp, mate),
    )
    po_copy.start()
    mine = span(core * half_rows, half_rows, half_rows)
    base = x_ref[mine, :].astype(F32) + po_s[mine, :].astype(F32)
    po_copy.wait_recv()
    middle = base + po_r[...].astype(F32)
    mid[...] = middle
    scaled = lax.rsqrt(jnp.mean(middle * middle, axis=1, keepdims=True) + eps_norm)
    normed = (middle * scaled * fg_ref[...]).astype(BF)

    def slot(k, c):
        return allnorm.at[span(k * rows + c * half_rows, half_rows, half_rows)]

    allnorm[span(in_group * rows + core * half_rows, half_rows, half_rows), :] = normed

    wide = normed.astype(F32)
    pieces = width // LANES

    def halo_fill(row):
        for k in range(pieces):
            halo_s[k : k + 1, :] = wide[row : row + 1, k * LANES : (k + 1) * LANES]

    def halo_copy(k):
        other = (1 - half_at) * group
        return remote(
            halo_s, halo_r, h_ss.at[k], h_rs.at[0], (other + k // 2, lax.rem(k, 2))
        )

    sends_first = jnp.logical_and(jnp.logical_and(half_at == 1, in_group == 0), core == 0)
    sends_last = jnp.logical_and(jnp.logical_and(half_at == 0, in_group == group - 1), core == 1)

    @pl.when(sends_first)
    def _():
        halo_fill(0)

    @pl.when(sends_last)
    def _():
        halo_fill(half_rows - 1)

    sends = jnp.logical_or(sends_first, sends_last)

    @pl.when(sends)
    def _():
        loop(0, 2 * group, lambda k: halo_copy(k).start())

    def ag_copy(d):
        t = g_base + lax.rem(in_group + d, group)
        return remote(
            slot(in_group, core), slot(in_group, core), ag_ss.at[d], ag_rs.at[d], (t, core)
        )

    def fw_copy(d):
        s = lax.rem(in_group + group - d, group)
        return remote(slot(s, core), slot(s, core), fw_ss.at[d], fw_rs.at[d], (sp, mate))

    loop(1, group, lambda d: ag_copy(d).start())
    fw_copy(0).start()

    def ag_wait(d):
        s = lax.rem(in_group + group - d, group)
        remote(slot(s, core), slot(s, core), ag_ss.at[d], ag_rs.at[d], (sp, mate)).wait_recv()
        fw_copy(d).start()

    own_w.wait()

    def w_wait(d):
        s = lax.rem(sp + n - d, n)
        dst = wrecv.at[:, lane_block(s)]
        remote(dst, dst, w_ss.at[d], w_rs.at[d], (s, core)).wait_recv()

    loop(1, n, w_wait)

    def up(block):
        both = nt(block, wrecv[: 2 * units, :]).astype(BF).astype(F32)
        return both[:, :units], both[:, units:]

    def up_rows(d):
        s = lax.rem(in_group + group - d, group)

        @pl.when(d > 0)
        def _():
            ag_wait(d)

        remote(slot(s, mate), slot(s, mate), fw_ss.at[d], fw_rs.at[d], (sp, mate)).wait_recv()
        gate, value = up(allnorm[span(s * rows, rows, rows), :])
        at = span(8 + s * rows, rows, 8)
        pre_g[at, :] = gate
        pre_v[at, :] = value

    loop(0, group, up_rows)
    remote(halo_r, halo_r, h_ss.at[0], h_rs.at[0], (sp, mate)).wait_recv()
    edge = jnp.concatenate([halo_r[k : k + 1, :] for k in range(pieces)], axis=1)
    gate, value = up(jnp.broadcast_to(edge, (16, width)).astype(BF))
    span_rows = group * rows
    zeros = jnp.zeros((8, units), F32)
    pre_g[:8, :] = jnp.where(half_at == 1, gate[:8], zeros)
    pre_v[:8, :] = jnp.where(half_at == 1, value[:8], zeros)
    pre_g[8 + span_rows :, :] = jnp.where(half_at == 0, gate[:8], zeros)
    pre_v[8 + span_rows :, :] = jnp.where(half_at == 0, value[:8], zeros)

    def convolve(ref, taps, k):
        block = ref[span(k * rows, rows + 16, 8), :]
        return (
            taps[0:1, :] * block[7 : 7 + rows]
            + taps[1:2, :] * block[8 : 8 + rows]
            + taps[2:3, :] * block[9 : 9 + rows]
        )

    def dd_copy(d):
        return remote(
            part.at[d, span(mate * half_rows, half_rows, half_rows)], ddbuf.at[d],
            dd_ss.at[d], dd_rs.at[d], (sp, mate),
        )

    def c_copy(d):
        t = g_base + lax.rem(in_group + d, group)
        return remote(rs_s.at[d], rs_r.at[d], c_ss.at[d], c_rs.at[d], (t, core))

    def combine(d):
        dd_copy(d).wait_recv()
        return part[d, mine, :].astype(F32) + ddbuf[d].astype(F32)

    def send_sum(d):
        rs_s[d] = combine(d).astype(BF)
        c_copy(d).start()

    def down(d):
        k = lax.rem(in_group + d, group)
        gate = convolve(pre_g, cg_ref, k)
        value = convolve(pre_v, cv_ref, k)
        hidden = (gate / (1.0 + jnp.exp(-gate)) * value).astype(BF)
        e = lax.rem(d, group)
        part[e] = jnp.dot(hidden, wrecv[2 * units :, :], preferred_element_type=F32).astype(BF)
        dd_copy(e).start()

        @pl.when(d > 1)
        def _():
            send_sum(d - 1)

    loop(1, group + 1, down)
    own_sum[...] = mid[...] + combine(0)

    def add_in(d):
        remote(rs_r.at[d], rs_r.at[d], c_ss.at[d], c_rs.at[d], (sp, mate)).wait_recv()
        own_sum[...] = own_sum[...] + rs_r[d].astype(F32)

    loop(1, group, add_in)
    fin_s[...] = own_sum[...].astype(BF)
    fin_copy = remote(fin_s, fin_r, fin_sem.at[0], fin_sem.at[1], (sp, mate))
    fin_copy.start()
    out_ref[mine, :] = fin_s[...]

    loop(1, kv_heads, lambda d: q_copy(d).wait_send())
    loop(1, n, lambda d: kv_copy(d).wait_send())
    loop(1, n, lambda d: w_copy(d).wait_send())
    loop(1, kv_heads, lambda d: o_copy(d).wait_send())
    po_copy.wait_send()
    loop(1, group, lambda d: ag_copy(d).wait_send())
    loop(0, group, lambda d: fw_copy(d).wait_send())

    @pl.when(sends)
    def _():
        loop(0, 2 * group, lambda k: halo_copy(k).wait_send())

    loop(0, group, lambda d: dd_copy(d).wait_send())
    loop(1, group, lambda d: c_copy(d).wait_send())
    fin_copy.wait_send()
    fin_copy.wait_recv()
    out_ref[span(mate * half_rows, half_rows, half_rows), :] = fin_r[...]


def rotary_tables(count):
    lanes = jnp.arange(LANES)
    length = HEAD_SIZE // 2
    rate_at = (lanes % (length // 2)).astype(F32)
    rates = 1.0 / theta ** (rate_at * 2.0 / length)
    angles = jnp.arange(count, dtype=F32)[:, None] * rates[None, :]
    sign = jnp.where(lanes % length < length // 2, -1.0, 1.0)
    return jnp.cos(angles), jnp.sin(angles) * sign[None, :]


def kernel_shards(
    n, halves, x_rows, queries, keys, values, query_norm_gain, key_norm_gain, out_weight, ffn_gain,
    gate_weight, value_weight, conv_gate, conv_value, down_weight,
):
    rows, width = x_rows.shape
    kv_heads = keys.shape[1] // HEAD_SIZE
    group = n // halves
    unit_local = gate_weight.shape[1]
    units = unit_local // group
    depth = gate_weight.shape[0]
    kv = jnp.concatenate(
        [keys.reshape(rows, kv_heads, HEAD_SIZE), values.reshape(rows, kv_heads, HEAD_SIZE)], axis=-1
    ).reshape(rows, kv_heads * LANES)
    turned = [
        w.T.reshape(group, units, depth) for w in (gate_weight, value_weight, down_weight)
    ]
    weights = jnp.concatenate(turned, axis=1)
    chip = lax.rem(lax.axis_index("sp"), group)
    taps = [lax.dynamic_slice_in_dim(t, chip * units, units, 1) for t in (conv_gate, conv_value)]
    cos, sin = rotary_tables(max(GRID_ROW_WIDTH, n * rows // GRID_ROW_WIDTH))
    tokens, q_tokens, span_rows = n * rows, kv_heads * rows, group * rows
    half_rows = rows // 2
    dma = pltpu.SemaphoreType.DMA
    vm = pltpu.VMEM
    scratch = [
        vm((tokens, LANES), BF), vm((q_tokens, LANES), BF), vm((tokens, 2 * LANES), BF),
        vm((2 * q_tokens, LANES), BF), vm((q_tokens, LANES), BF), vm((rows, kv_heads * LANES), BF),
        vm((rows, width), BF), vm((half_rows, width), BF), vm((half_rows, width), F32),
        vm((span_rows, width), BF), vm((width // LANES, LANES), F32),
        vm((width // LANES, LANES), F32), vm((3 * units, width), BF),
        vm((span_rows + 16, units), F32), vm((span_rows + 16, units), F32),
        vm((group, rows, width), BF), vm((group, half_rows, width), BF),
        vm((half_rows, width), F32), vm((group, half_rows, width), BF),
        vm((group, half_rows, width), BF), vm((half_rows, width), BF), vm((half_rows, width), BF),
        dma((3,)), dma((n,)), dma((n,)), dma((kv_heads,)), dma((kv_heads,)), dma((n,)), dma((n,)),
        dma((kv_heads,)), dma((kv_heads,)), dma((2,)), dma((group,)), dma((group,)),
        dma((group,)), dma((group,)), dma((2 * group,)), dma((1,)), dma((group,)), dma((group,)),
        dma((group,)), dma((group,)), dma((2,)),
    ]
    args = (
        x_rows, queries, kv, jnp.tile(query_norm_gain, 2)[None, :], jnp.tile(key_norm_gain, 2)[None, :],
        cos, sin, out_weight, ffn_gain[None, :], weights, taps[0], taps[1],
    )
    return pl.pallas_call(
        lambda *refs: layer_kernel(n, halves, *refs),
        out_shape=jax.ShapeDtypeStruct((rows, width), BF),
        in_specs=[pl.BlockSpec(memory_space=pltpu.VMEM)] * len(args),
        out_specs=pl.BlockSpec(memory_space=pltpu.VMEM),
        scratch_shapes=scratch,
        compiler_params=pltpu.CompilerParams(
            collective_id=0, has_side_effects=True, vmem_limit_bytes=60 * 2**20
        ),
        name="layer",
    )(*args)


def suits(mesh, sizes):
    n, pair = mesh.shape["sp"], mesh.shape["tp"]
    x_rows, queries, keys, gate = sizes
    if pair != 2 or n % 2:
        return False
    rows, group = x_rows[0] // n, n // 2
    heads = keys[1] // pair // HEAD_SIZE
    units = gate[1] // pair
    return (
        rows % GRID_ROW_WIDTH == 0
        and rows % 32 == 0
        and queries[1] == 2 * keys[1]
        and n % heads == 0
        and 2 * HEAD_SIZE == LANES
        and x_rows[1] == n * LANES
        and units % (16 * group) == 0
    )


def solution(mesh):
    placed = (
        P("sp", None),
        P("sp", "tp"),
        P("sp", "tp"),
        P("sp", "tp"),
        P(),
        P(),
        P("tp", None),
        P(),
        P("sp", "tp"),
        P("sp", "tp"),
        P(None, "tp"),
        P(None, "tp"),
        P("sp", "tp"),
    )
    def run(*arrays):
        n = mesh.shape["sp"]
        fits = suits(mesh, [arrays[k].shape for k in (0, 1, 2, 8)])
        local = functools.partial(kernel_shards, n, 2) if fits else shards
        return jax.shard_map(
            local, mesh=mesh, in_specs=placed, out_specs=P("sp", None), check_vma=False
        )(*arrays)

    return run
```

```python
import functools
import math

import jax
import jax.numpy as jnp
from jax import lax
from jax.experimental import pallas as pl
from jax.experimental.pallas import tpu as pltpu
from jax.sharding import PartitionSpec as P

HEAD_SIZE = 64
GRID_ROW_WIDTH = 64


eps_norm = 1e-06
theta = 10000.0


def with_halo(cells, sides, width):
    for axis, dim in sides:
        count = lax.axis_size(axis)
        ends = count - 1
        head = lax.slice_in_dim(cells, 0, width, axis=dim)
        tail = lax.slice_in_dim(cells, cells.shape[dim] - width, cells.shape[dim], axis=dim)
        cells = jnp.concatenate(
            [
                lax.ppermute(tail, axis, [(i, (i + 1) % count) for i in range(ends)]),
                cells,
                lax.ppermute(head, axis, [((i + 1) % count, i) for i in range(ends)]),
            ],
            axis=dim,
        )
    return cells


def per_head_norm(head_block, gain_vec):
    wide_vals = head_block.astype(jnp.float32)
    inverse_rms = lax.rsqrt(jnp.mean(wide_vals * wide_vals, axis=-1, keepdims=True) + eps_norm)
    return wide_vals * inverse_rms * gain_vec


def turn_half(half_vec, places):
    quarter_len = half_vec.shape[-1] // 2
    inverse_rates = 1.0 / theta ** (
        jnp.arange(quarter_len, dtype=jnp.float32) * 2.0 / half_vec.shape[-1]
    )
    angles = places.astype(jnp.float32)[:, None] * inverse_rates[None, :]
    angles = jnp.concatenate([angles, angles], axis=-1)[:, None, :]
    front_part = half_vec[..., :quarter_len]
    back_part = half_vec[..., quarter_len:]
    return half_vec * jnp.cos(angles) + jnp.concatenate(
        [-back_part, front_part], axis=-1
    ) * jnp.sin(angles)


def apply_rotary(normed_heads, token_positions):
    half_point = normed_heads.shape[-1] // 2
    grid_row = token_positions // GRID_ROW_WIDTH
    grid_col = token_positions % GRID_ROW_WIDTH
    return jnp.concatenate(
        [
            turn_half(normed_heads[..., :half_point], grid_row),
            turn_half(normed_heads[..., half_point:], grid_col),
        ],
        axis=-1,
    )


def row_norm(rows_wide, gain_vec):
    inverse_rms = lax.rsqrt(jnp.mean(rows_wide * rows_wide, axis=-1, keepdims=True) + eps_norm)
    return (rows_wide * inverse_rms * gain_vec).astype(jnp.bfloat16)


def contract_units(left_rows, right_rows):
    return lax.dot_general(
        left_rows, right_rows, (((1,), (1,)), ((), ())), preferred_element_type=jnp.float32
    )


def shards(
    x_rows,
    queries,
    keys,
    values,
    query_norm_gain,
    key_norm_gain,
    out_weight,
    ffn_gain,
    gate_weight,
    value_weight,
    conv_gate,
    conv_value,
    down_weight,
):
    collected = (
        lax.all_gather(gate_weight, "sp", axis=0, tiled=True),
        lax.all_gather(value_weight, "sp", axis=0, tiled=True),
        lax.all_gather(down_weight, "sp", axis=0, tiled=True),
    )
    tokens_here = queries.shape[0]
    query_heads = queries.shape[1] // HEAD_SIZE
    key_heads = keys.shape[1] // HEAD_SIZE
    group_width = query_heads // key_heads
    lane_rows = group_width * tokens_here
    token_positions = lax.axis_index("sp") * tokens_here + jnp.arange(tokens_here, dtype=jnp.int32)
    rotated_queries = apply_rotary(
        per_head_norm(queries.reshape(tokens_here, query_heads, HEAD_SIZE), query_norm_gain),
        token_positions,
    )
    query_lanes = rotated_queries.reshape(tokens_here, key_heads, group_width, HEAD_SIZE).transpose(
        1, 2, 0, 3
    )
    query_lanes = query_lanes.reshape(key_heads, lane_rows, HEAD_SIZE) * HEAD_SIZE ** (-0.5)
    start_state = (
        jnp.full((key_heads, lane_rows), -1e30, jnp.float32),
        jnp.zeros((key_heads, lane_rows), jnp.float32),
        jnp.zeros((key_heads, lane_rows, HEAD_SIZE), jnp.float32),
    )
    key_piece = lax.all_gather(keys, "sp", axis=0, tiled=True)
    value_piece = lax.all_gather(values, "sp", axis=0, tiled=True)
    row_count = key_piece.shape[0]
    key_places = jnp.arange(row_count, dtype=jnp.int32)
    turned = apply_rotary(
        per_head_norm(key_piece.reshape(row_count, key_heads, HEAD_SIZE), key_norm_gain), key_places
    )
    key_span = math.gcd(row_count, 2048)
    span_count = row_count // key_span
    turned = turned.reshape(span_count, key_span, key_heads, HEAD_SIZE)
    value_matrix = value_piece.reshape(span_count, key_span, key_heads, HEAD_SIZE)

    def one_span(state_now, inputs):
        running_top, denominator, weighted = state_now
        key_block, value_block = inputs
        scores = jnp.einsum("hrd,shd->hrs", query_lanes, key_block, precision=lax.Precision.HIGHEST)
        new_top = jnp.maximum(running_top, jnp.max(scores, axis=-1))
        factor = jnp.exp(running_top - new_top)
        weights = jnp.exp(scores - new_top[..., None])
        denominator = denominator * factor + jnp.sum(weights, axis=-1)
        weighted = weighted * factor[..., None] + jnp.einsum(
            "hrs,shd->hrd",
            weights.astype(jnp.bfloat16),
            value_block,
            preferred_element_type=jnp.float32,
        )
        return ((new_top, denominator, weighted), None)

    folded_state, _ = lax.scan(one_span, start_state, (turned, value_matrix))
    running_top, denominator, weighted = folded_state
    attended = (weighted / denominator[..., None]).reshape(
        key_heads, group_width, tokens_here, HEAD_SIZE
    )
    attended = (
        attended.transpose(2, 0, 1, 3)
        .reshape(tokens_here, query_heads * HEAD_SIZE)
        .astype(jnp.bfloat16)
    )
    share_rows = tokens_here // lax.axis_size("tp")
    head_share = lax.psum_scatter(
        jnp.dot(attended, out_weight, preferred_element_type=jnp.float32).astype(jnp.bfloat16),
        "tp",
        scatter_dimension=0,
        tiled=True,
    ).astype(jnp.float32)
    own_rows = lax.dynamic_slice_in_dim(x_rows, lax.axis_index("tp") * share_rows, share_rows, 0)
    middle_rows = own_rows.astype(jnp.float32) + head_share
    normed = lax.all_gather(row_norm(middle_rows, ffn_gain), "tp", axis=0, tiled=True)
    unit_local = gate_weight.shape[1]
    gate_pre = jnp.dot(normed, collected[0], preferred_element_type=jnp.float32).astype(
        jnp.bfloat16
    )
    value_pre = jnp.dot(normed, collected[1], preferred_element_type=jnp.float32).astype(
        jnp.bfloat16
    )
    joined = jnp.concatenate([gate_pre, value_pre], axis=1)
    padded = with_halo(joined, (("sp", 0),), 1).astype(jnp.float32)
    conv_taps = jnp.concatenate([conv_gate, conv_value], axis=1)
    convolved = conv_taps[0] * padded[:-2] + conv_taps[1] * padded[1:-1] + conv_taps[2] * padded[2:]
    hidden = (jax.nn.silu(convolved[:, :unit_local]) * convolved[:, unit_local:]).astype(
        jnp.bfloat16
    )
    unit_share = lax.psum_scatter(
        contract_units(hidden, collected[2]).astype(jnp.bfloat16),
        "tp",
        scatter_dimension=0,
        tiled=True,
    ).astype(jnp.float32)
    finished = (middle_rows + unit_share).astype(jnp.bfloat16)
    return lax.all_gather(finished, "tp", axis=0, tiled=True)

LANES = 128
MESH = pl.DeviceIdType.MESH
BF = jnp.bfloat16
F32 = jnp.float32


def rem(a, b):
    return a % b if isinstance(a, int) else lax.rem(a, b)


def nt(left, right):
    return lax.dot_general(left, right, (((1,), (1,)), ((), ())), preferred_element_type=F32)


def layer_kernel(
    n, x_ref, q_ref, kv_ref, qg_ref, kg_ref, cos_ref, sin_ref, wo_ref, fg_ref, w_ref,
    cg_ref, cv_ref, out_ref,
    kvbuf, qbuf, kcat, qcat, att_s, attbuf, po_s, po_r, mid, allnorm, edge_s, edge_r, wrecv,
    pre_g, pre_v, part, ddbuf, own_sum, rs_s, rs_r, fin_s, fin_r,
    loc, kv_ss, kv_rs, q_ss, q_rs, w_ss, w_rs, wf_ss, wf_rs, dw_ss, dw_rs, df_ss, df_rs, o_ss, o_rs, po_sem, ag_ss, ag_rs, fw_ss, fw_rs,
    h_sem, dd_ss, dd_rs, c_ss, c_rs, fin_sem,
):
    sp = lax.axis_index("sp")
    core = lax.axis_index("tp")
    mate = 1 - core
    rows = x_ref.shape[0]
    half_rows = rows // 2
    width = x_ref.shape[1]
    kv_heads = kv_ref.shape[1] // LANES
    plane = n // 4
    group = 2 * plane
    tokens = n * rows
    q_tokens = kv_heads * rows
    units = w_ref.shape[1] // 3
    head_at = rem(sp, kv_heads)
    q_base = sp - head_at
    place = rem(sp, plane)
    side = rem(sp // plane, 2)
    wing = sp // (2 * plane)
    member = wing * plane + place

    def chip(m, at_side):
        return (m // plane) * (2 * plane) + at_side * plane + rem(m, plane)

    def ahead(d):
        return rem(wing + d // plane, 2) * plane + rem(place + rem(d, plane), plane)

    def behind(d):
        return rem(wing + d // plane, 2) * plane + rem(
            place + plane - rem(d, plane), plane
        )

    twin = chip(member, 1 - side)

    def remote(src, dst, ss, rs, device):
        return pltpu.make_async_remote_copy(
            src_ref=src, dst_ref=dst, send_sem=ss, recv_sem=rs, device_id=device, device_id_type=MESH
        )

    def lane_block(k):
        return pl.ds(pl.multiple_of(k * LANES, LANES), LANES)

    def span(start, size, unit):
        return pl.ds(pl.multiple_of(start, unit), size)

    def loop(lo, hi, fn):
        def step(k, carry):
            fn(k)
            return carry

        lax.fori_loop(lo, hi, step, 0)

    barrier = pltpu.get_barrier_semaphore()

    def greet(d):
        t = rem(sp + d, n)
        pl.semaphore_signal(barrier, inc=1, device_id=(t, core), device_id_type=MESH)
        pl.semaphore_signal(barrier, inc=1, device_id=(t, mate), device_id_type=MESH)

    loop(1, n, greet)
    pl.semaphore_signal(barrier, inc=1, device_id=(sp, mate), device_id_type=MESH)
    pl.semaphore_wait(barrier, 2 * n - 1)

    def q_copy(d):
        t = q_base + rem(head_at + d, kv_heads)
        return remote(
            q_ref.at[:, lane_block(t - q_base)], qbuf.at[span(head_at * rows, rows, rows)],
            q_ss.at[d], q_rs.at[d], (t, core),
        )

    def kv_copy(d):
        t = rem(sp + d, n)
        return remote(
            kv_ref.at[:, lane_block(rem(t, kv_heads))], kvbuf.at[span(sp * rows, rows, rows)],
            kv_ss.at[d], kv_rs.at[d], (t, core),
        )

    up_part, down_part = slice(0, 2 * units), slice(2 * units, 3 * units)

    def w_copy(d, part_at, ss, rs):
        m = ahead(d)
        return remote(
            w_ref.at[m, part_at], wrecv.at[part_at, lane_block(sp)],
            ss.at[d], rs.at[d], (chip(m, side), core),
        )

    def twin_first(part_at, ss, rs):
        return remote(
            w_ref.at[member, part_at], wrecv.at[part_at, lane_block(sp)],
            ss.at[0], rs.at[0], (twin, core),
        )

    def twin_copy(d, part_at, ss, rs):
        at = wrecv.at[part_at, lane_block(chip(behind(d), side))]
        return remote(at, at, ss.at[d], rs.at[d], (twin, core))

    def pass_on(d, part_at, ss, rs, next_ss, next_rs):
        dst = wrecv.at[part_at, lane_block(chip(behind(d), side))]
        remote(dst, dst, ss.at[d], rs.at[d], (twin, core)).wait_recv()
        twin_copy(d, part_at, next_ss, next_rs).start()

    def twin_wait(d, part_at, ss, rs):
        dst = wrecv.at[part_at, lane_block(chip(behind(d), 1 - side))]
        remote(dst, dst, ss.at[d], rs.at[d], (twin, core)).wait_recv()

    gate_sems, gate_next = (w_ss, w_rs), (wf_ss, wf_rs)
    down_sems, down_next = (dw_ss, dw_rs), (df_ss, df_rs)

    own_q = pltpu.make_async_copy(
        q_ref.at[:, lane_block(head_at)], qbuf.at[span(head_at * rows, rows, rows)], loc.at[0]
    )
    own_kv = pltpu.make_async_copy(
        kv_ref.at[:, lane_block(head_at)], kvbuf.at[span(sp * rows, rows, rows)], loc.at[1]
    )
    own_w = pltpu.make_async_copy(w_ref.at[member], wrecv.at[:, lane_block(sp)], loc.at[2])
    own_q.start()
    own_kv.start()
    loop(1, kv_heads, lambda d: q_copy(d).start())
    loop(1, n, lambda d: kv_copy(d).start())
    loop(1, group, lambda d: w_copy(d, up_part, *gate_sems).start())
    twin_first(up_part, *gate_next).start()
    own_w.start()

    lane = lax.broadcasted_iota(jnp.int32, (GRID_ROW_WIDTH, LANES), 1)
    low = lane < HEAD_SIZE
    first = rem(lane, 2 * HEAD_SIZE // 4) < HEAD_SIZE // 4
    by_row = rem(lane, HEAD_SIZE) < HEAD_SIZE // 2

    def turn(vals, grid_row):
        cos = jnp.where(by_row, cos_ref[pl.ds(grid_row, 1), :], cos_ref[:GRID_ROW_WIDTH, :])
        sin = jnp.where(by_row, sin_ref[pl.ds(grid_row, 1), :], sin_ref[:GRID_ROW_WIDTH, :])
        quarter = HEAD_SIZE // 4
        swapped = jnp.where(
            first, pltpu.roll(vals, LANES - quarter, 1), pltpu.roll(vals, quarter, 1)
        )
        return vals * cos + swapped * sin

    def split(vals):
        top = vals.astype(BF).astype(F32)
        return top, (vals - top).astype(BF).astype(F32)

    def make_q(r):
        at = span(r * GRID_ROW_WIDTH, GRID_ROW_WIDTH, GRID_ROW_WIDTH)
        vals = qbuf[at, :].astype(F32)
        sq = vals * vals
        low_sum = jnp.sum(jnp.where(low, sq, 0.0), axis=1, keepdims=True)
        high_sum = jnp.sum(jnp.where(low, 0.0, sq), axis=1, keepdims=True)
        inverse = jnp.where(
            low,
            lax.rsqrt(low_sum * (1.0 / HEAD_SIZE) + eps_norm),
            lax.rsqrt(high_sum * (1.0 / HEAD_SIZE) + eps_norm),
        )
        turned = turn(vals * inverse * qg_ref[...], q_base * (rows // GRID_ROW_WIDTH) + r)
        top, rest = split(turned * HEAD_SIZE ** (-0.5))
        qcat[at, :] = jnp.where(low, top, pltpu.roll(rest, HEAD_SIZE, 1)).astype(BF)
        later = span(q_tokens + r * GRID_ROW_WIDTH, GRID_ROW_WIDTH, GRID_ROW_WIDTH)
        qcat[later, :] = jnp.where(low, pltpu.roll(top, HEAD_SIZE, 1), rest).astype(BF)

    own_q.wait()

    def q_take(d):
        s = rem(head_at + kv_heads - d, kv_heads)
        dst = qbuf.at[span(s * rows, rows, rows)]

        @pl.when(d > 0)
        def _():
            remote(dst, dst, q_ss.at[d], q_rs.at[d], (q_base + s, core)).wait_recv()

        for r in range(rows // GRID_ROW_WIDTH):
            make_q(s * (rows // GRID_ROW_WIDTH) + r)

    loop(0, kv_heads, q_take)
    steps = rows // GRID_ROW_WIDTH

    def make_k(r):
        at = span(r * GRID_ROW_WIDTH, GRID_ROW_WIDTH, GRID_ROW_WIDTH)
        vals = kvbuf[at, :].astype(F32)
        total = jnp.sum(jnp.where(low, vals * vals, 0.0), axis=1, keepdims=True)
        turned = turn(
            vals * lax.rsqrt(total * (1.0 / HEAD_SIZE) + eps_norm) * kg_ref[...], r
        )
        top, rest = split(turned)
        kcat[at, :LANES] = jnp.where(low, top, pltpu.roll(top, HEAD_SIZE, 1)).astype(BF)
        kcat[at, LANES:] = jnp.where(low, rest, pltpu.roll(rest, HEAD_SIZE, 1)).astype(BF)

    own_kv.wait()

    def kv_take(d):
        s = rem(sp + n - d, n)
        dst = kvbuf.at[span(s * rows, rows, rows)]

        @pl.when(d > 0)
        def _():
            remote(dst, dst, kv_ss.at[d], kv_rs.at[d], (s, core)).wait_recv()

        for r in range(steps):
            make_k(s * steps + r)

    loop(0, n, kv_take)
    loop(1, plane, lambda d: pass_on(d, up_part, *gate_sems, *gate_next))

    def o_copy(d):
        k = rem(head_at + d, kv_heads)
        return remote(
            att_s.at[span(k * rows, rows, rows)], attbuf.at[:, lane_block(head_at)],
            o_ss.at[d], o_rs.at[d], (q_base + k, core),
        )

    low_rows = lax.broadcasted_iota(jnp.int32, (rows, LANES), 1) < HEAD_SIZE

    def attend(k):
        both = jnp.concatenate(
            [qcat[span(k * rows, rows, rows), :], qcat[span(q_tokens + k * rows, rows, rows), :]],
            axis=0,
        )
        scores = nt(jnp.concatenate([both, both], axis=1), kcat[...])
        shifted = jnp.exp(scores - jnp.max(scores, axis=1, keepdims=True))
        total = jnp.sum(shifted, axis=1, keepdims=True)
        summed = jnp.dot(shifted.astype(BF), kvbuf[...], preferred_element_type=F32) / total
        return jnp.where(
            low_rows, pltpu.roll(summed[:rows], HEAD_SIZE, 1), summed[rows:]
        ).astype(BF)

    def attend_send(d):
        k = rem(head_at + d, kv_heads)
        att_s[span(k * rows, rows, rows), :] = attend(k)

        @pl.when(d < kv_heads)
        def _():
            o_copy(d).start()

    loop(1, kv_heads + 1, attend_send)
    attbuf[:, lane_block(head_at)] = att_s[span(head_at * rows, rows, rows), :]

    def o_wait(d):
        s = rem(head_at + kv_heads - d, kv_heads)
        dst = attbuf.at[:, lane_block(s)]
        remote(dst, dst, o_ss.at[d], o_rs.at[d], (q_base + s, core)).wait_recv()

    loop(1, kv_heads, o_wait)

    po_s[...] = jnp.dot(attbuf[...], wo_ref[...], preferred_element_type=F32).astype(BF)
    po_copy = remote(
        po_s.at[span(mate * half_rows, half_rows, half_rows)], po_r, po_sem.at[0], po_sem.at[1],
        (sp, mate),
    )
    po_copy.start()
    mine = span(core * half_rows, half_rows, half_rows)
    base = x_ref[mine, :].astype(F32) + po_s[mine, :].astype(F32)
    po_copy.wait_recv()
    middle = base + po_r[...].astype(F32)
    mid[...] = middle
    scaled = lax.rsqrt(jnp.mean(middle * middle, axis=1, keepdims=True) + eps_norm)
    normed = (middle * scaled * fg_ref[...]).astype(BF)

    def slot(k, c):
        return allnorm.at[span(k * rows + c * half_rows, half_rows, half_rows)]

    allnorm[span(member * rows + core * half_rows, half_rows, half_rows), :] = normed

    def ag_copy(d):
        to = ahead(rem(d, plane)) if d != plane else ahead(d)
        of = member if d <= plane else (1 - wing) * plane + place
        return remote(
            slot(of, core), slot(of, core), ag_ss.at[d], ag_rs.at[d], (chip(to, side), core)
        )

    def fw_copy(d):
        s = behind(d)
        return remote(slot(s, core), slot(s, core), fw_ss.at[d], fw_rs.at[d], (sp, mate))

    def ag_wait(d):
        s = behind(d)
        remote(slot(s, core), slot(s, core), ag_ss.at[d], ag_rs.at[d], (sp, mate)).wait_recv()
        fw_copy(d).start()

    ag_copy(plane).start()
    for d in range(1, plane):
        ag_copy(d).start()
    fw_copy(0).start()
    loop(1, group, lambda d: w_copy(d, down_part, *down_sems).start())
    twin_first(down_part, *down_next).start()

    own_w.wait()
    loop(plane, group, lambda d: pass_on(d, up_part, *gate_sems, *gate_next))
    ag_wait(plane)
    for d in range(plane + 1, group):
        ag_copy(d).start()
    loop(0, group, lambda d: twin_wait(d, up_part, *gate_next))

    def up(block):
        both = nt(block, wrecv[: 2 * units, :]).astype(BF).astype(F32)
        return both[:, :units], both[:, units:]

    seg = plane * rows
    pitch = seg + 16

    def row_of(m):
        return (m // plane) * pitch + rem(m, plane) * rows

    def up_rows(d):
        s = behind(d)

        @pl.when(jnp.logical_and(d > 0, d != plane))
        def _():
            ag_wait(d)

        remote(slot(s, mate), slot(s, mate), fw_ss.at[d], fw_rs.at[d], (sp, mate)).wait_recv()
        gate, value = up(allnorm[span(s * rows, rows, rows), :])
        at = span(row_of(s) + 8, rows, 8)
        pre_g[at, :] = gate
        pre_v[at, :] = value

    loop(0, plane + 1, up_rows)
    loop(1, group, lambda d: pass_on(d, down_part, *down_sems, *down_next))
    loop(plane + 1, group, up_rows)

    edge_at = (8, 8 + seg - 1, pitch + 8, pitch + 8 + seg - 1)
    edge_s[...] = jnp.concatenate(
        [
            jnp.concatenate([pre[k : k + 1, :] for k in edge_at] * 2, axis=0)
            for pre in (pre_g, pre_v)
        ],
        axis=0,
    )
    edge_copy = remote(edge_s, edge_r, h_sem.at[0], h_sem.at[1], (twin, core))
    edge_copy.start()
    loop(0, group, lambda d: twin_wait(d, down_part, *down_next))
    edge_copy.wait_recv()
    for pre, first_row in ((pre_g, 0), (pre_v, 8)):
        near = [
            jnp.broadcast_to(edge_r[first_row + k : first_row + k + 1, :], (8, units))
            for k in range(4)
        ]
        none = jnp.zeros((8, units), F32)
        pre[0:8, :] = jnp.where(side == 0, none, near[1])
        pre[8 + seg : pitch, :] = jnp.where(side == 0, near[0], near[2])
        pre[pitch : pitch + 8, :] = jnp.where(side == 0, near[1], near[3])
        pre[pitch + 8 + seg :, :] = jnp.where(side == 0, near[2], none)

    def convolve(ref, taps, k):
        block = ref[span(row_of(k), rows + 16, 8), :]
        return (
            taps[0:1, :] * block[7 : 7 + rows]
            + taps[1:2, :] * block[8 : 8 + rows]
            + taps[2:3, :] * block[9 : 9 + rows]
        )

    def dd_copy(d):
        return remote(
            part.at[d, span(mate * half_rows, half_rows, half_rows)], ddbuf.at[d],
            dd_ss.at[d], dd_rs.at[d], (sp, mate),
        )

    def c_copy(d, to):
        return remote(rs_s.at[d], rs_r.at[d], c_ss.at[d], c_rs.at[d], (chip(to, side), core))

    def c_near(d):
        return c_copy(d, ahead(rem(d, plane)))

    def combine(d):
        dd_copy(d).wait_recv()
        return part[d, mine, :].astype(F32) + ddbuf[d].astype(F32)

    def send_sum(d):
        rs_s[d] = combine(d).astype(BF)
        c_near(d).start()

    def order(j):
        return plane * (1 - j // plane) + rem(j + 1, plane)

    def down(j):
        d = order(j)
        k = ahead(d)
        gate = convolve(pre_g, cg_ref, k)
        value = convolve(pre_v, cv_ref, k)
        hidden = (gate / (1.0 + jnp.exp(-gate)) * value).astype(BF)
        part[d] = jnp.dot(hidden, wrecv[2 * units :, :], preferred_element_type=F32).astype(BF)
        dd_copy(d).start()
        last = order(jnp.maximum(j - 1, 0))

        @pl.when(jnp.logical_and(j > 0, rem(last, plane) > 0))
        def _():
            send_sum(last)

    loop(0, group, down)

    def add_in(d):
        remote(rs_r.at[d], rs_r.at[d], c_ss.at[d], c_rs.at[d], (sp, mate)).wait_recv()
        own_sum[...] = own_sum[...] + rs_r[d].astype(F32)

    own_sum[...] = combine(plane)
    loop(plane + 1, group, add_in)
    rs_s[plane] = own_sum[...].astype(BF)
    far_copy = c_copy(plane, (1 - wing) * plane + place)
    far_copy.start()
    own_sum[...] = mid[...] + combine(0)
    loop(1, plane + 1, add_in)
    fin_s[...] = own_sum[...].astype(BF)
    fin_copy = remote(fin_s, fin_r, fin_sem.at[0], fin_sem.at[1], (sp, mate))
    fin_copy.start()
    out_ref[mine, :] = fin_s[...]

    loop(1, kv_heads, lambda d: q_copy(d).wait_send())
    loop(1, n, lambda d: kv_copy(d).wait_send())
    loop(1, group, lambda d: w_copy(d, up_part, *gate_sems).wait_send())
    loop(1, group, lambda d: w_copy(d, down_part, *down_sems).wait_send())
    loop(0, group, lambda d: twin_copy(d, up_part, *gate_next).wait_send())
    loop(0, group, lambda d: twin_copy(d, down_part, *down_next).wait_send())
    loop(1, kv_heads, lambda d: o_copy(d).wait_send())
    po_copy.wait_send()
    for d in range(1, group):
        ag_copy(d).wait_send()
    loop(0, group, lambda d: fw_copy(d).wait_send())
    edge_copy.wait_send()
    loop(0, group, lambda d: dd_copy(d).wait_send())
    loop(1, plane, lambda d: c_near(d).wait_send())
    loop(plane + 1, group, lambda d: c_near(d).wait_send())
    far_copy.wait_send()
    fin_copy.wait_send()
    fin_copy.wait_recv()
    out_ref[span(mate * half_rows, half_rows, half_rows), :] = fin_r[...]


def rotary_tables(count):
    lanes = jnp.arange(LANES)
    length = HEAD_SIZE // 2
    rate_at = (lanes % (length // 2)).astype(F32)
    rates = 1.0 / theta ** (rate_at * 2.0 / length)
    angles = jnp.arange(count, dtype=F32)[:, None] * rates[None, :]
    sign = jnp.where(lanes % length < length // 2, -1.0, 1.0)
    return jnp.cos(angles), jnp.sin(angles) * sign[None, :]


def kernel_shards(
    n, x_rows, queries, keys, values, query_norm_gain, key_norm_gain, out_weight, ffn_gain,
    gate_weight, value_weight, conv_gate, conv_value, down_weight,
):
    rows, width = x_rows.shape
    kv_heads = keys.shape[1] // HEAD_SIZE
    plane = n // 4
    group = 2 * plane
    unit_local = gate_weight.shape[1]
    units = unit_local // group
    depth = gate_weight.shape[0]
    kv = jnp.concatenate(
        [keys.reshape(rows, kv_heads, HEAD_SIZE), values.reshape(rows, kv_heads, HEAD_SIZE)], axis=-1
    ).reshape(rows, kv_heads * LANES)
    turned = [
        w.T.reshape(group, units, depth) for w in (gate_weight, value_weight, down_weight)
    ]
    weights = jnp.concatenate(turned, axis=1)
    at = lax.axis_index("sp")
    chip = (at // group) * plane + rem(at, plane)
    taps = [lax.dynamic_slice_in_dim(t, chip * units, units, 1) for t in (conv_gate, conv_value)]
    cos, sin = rotary_tables(max(GRID_ROW_WIDTH, n * rows // GRID_ROW_WIDTH))
    tokens, q_tokens, span_rows = n * rows, kv_heads * rows, group * rows
    half_rows = rows // 2
    dma = pltpu.SemaphoreType.DMA
    vm = pltpu.VMEM
    scratch = [
        vm((tokens, LANES), BF), vm((q_tokens, LANES), BF), vm((tokens, 2 * LANES), BF),
        vm((2 * q_tokens, LANES), BF), vm((q_tokens, LANES), BF), vm((rows, kv_heads * LANES), BF),
        vm((rows, width), BF), vm((half_rows, width), BF), vm((half_rows, width), F32),
        vm((span_rows, width), BF), vm((16, units), F32),
        vm((16, units), F32), vm((3 * units, width), BF),
        vm((span_rows + 32, units), F32), vm((span_rows + 32, units), F32),
        vm((group, rows, width), BF), vm((group, half_rows, width), BF),
        vm((half_rows, width), F32), vm((group, half_rows, width), BF),
        vm((group, half_rows, width), BF), vm((half_rows, width), BF), vm((half_rows, width), BF),
        dma((3,)), dma((n,)), dma((n,)), dma((kv_heads,)), dma((kv_heads,)), *[dma((group,))] * 8,
        dma((kv_heads,)), dma((kv_heads,)), dma((2,)), dma((group,)), dma((group,)),
        dma((group,)), dma((group,)), dma((2,)), dma((group,)), dma((group,)),
        dma((group,)), dma((group,)), dma((2,)),
    ]
    args = (
        x_rows, queries, kv, jnp.tile(query_norm_gain, 2)[None, :], jnp.tile(key_norm_gain, 2)[None, :],
        cos, sin, out_weight, ffn_gain[None, :], weights, taps[0], taps[1],
    )
    return pl.pallas_call(
        lambda *refs: layer_kernel(n, *refs),
        out_shape=jax.ShapeDtypeStruct((rows, width), BF),
        in_specs=[pl.BlockSpec(memory_space=pltpu.VMEM)] * len(args),
        out_specs=pl.BlockSpec(memory_space=pltpu.VMEM),
        scratch_shapes=scratch,
        compiler_params=pltpu.CompilerParams(
            collective_id=0, has_side_effects=True, vmem_limit_bytes=60 * 2**20
        ),
        name="layer",
    )(*args)


def suits(mesh, sizes):
    n, pair = mesh.shape["sp"], mesh.shape["tp"]
    x_rows, queries, keys, gate = sizes
    if pair != 2 or n % 4:
        return False
    rows, group = x_rows[0] // n, n // 2
    heads = keys[1] // pair // HEAD_SIZE
    units = gate[1] // pair
    return (
        rows % GRID_ROW_WIDTH == 0
        and rows % 32 == 0
        and queries[1] == 2 * keys[1]
        and n % heads == 0
        and 2 * HEAD_SIZE == LANES
        and x_rows[1] == n * LANES
        and units % (16 * group) == 0
    )


def solution(mesh):
    placed = (
        P("sp", None),
        P("sp", "tp"),
        P("sp", "tp"),
        P("sp", "tp"),
        P(),
        P(),
        P("tp", None),
        P(),
        P("sp", "tp"),
        P("sp", "tp"),
        P(None, "tp"),
        P(None, "tp"),
        P("sp", "tp"),
    )
    def run(*arrays):
        n = mesh.shape["sp"]
        fits = suits(mesh, [arrays[k].shape for k in (0, 1, 2, 8)])
        local = functools.partial(kernel_shards, n) if fits else shards
        return jax.shard_map(
            local, mesh=mesh, in_specs=placed, out_specs=P("sp", None), check_vma=False
        )(*arrays)

    return run
```

```python
import functools
import math

import jax
import jax.numpy as jnp
from jax import lax
from jax.experimental import pallas as pl
from jax.experimental.pallas import tpu as pltpu
from jax.sharding import PartitionSpec as P

HEAD_SIZE = 64
GRID_ROW_WIDTH = 64


eps_norm = 1e-06
theta = 10000.0


def with_halo(cells, sides, width):
    for axis, dim in sides:
        count = lax.axis_size(axis)
        ends = count - 1
        head = lax.slice_in_dim(cells, 0, width, axis=dim)
        tail = lax.slice_in_dim(cells, cells.shape[dim] - width, cells.shape[dim], axis=dim)
        cells = jnp.concatenate(
            [
                lax.ppermute(tail, axis, [(i, (i + 1) % count) for i in range(ends)]),
                cells,
                lax.ppermute(head, axis, [((i + 1) % count, i) for i in range(ends)]),
            ],
            axis=dim,
        )
    return cells


def per_head_norm(head_block, gain_vec):
    wide_vals = head_block.astype(jnp.float32)
    inverse_rms = lax.rsqrt(jnp.mean(wide_vals * wide_vals, axis=-1, keepdims=True) + eps_norm)
    return wide_vals * inverse_rms * gain_vec


def turn_half(half_vec, places):
    quarter_len = half_vec.shape[-1] // 2
    inverse_rates = 1.0 / theta ** (
        jnp.arange(quarter_len, dtype=jnp.float32) * 2.0 / half_vec.shape[-1]
    )
    angles = places.astype(jnp.float32)[:, None] * inverse_rates[None, :]
    angles = jnp.concatenate([angles, angles], axis=-1)[:, None, :]
    front_part = half_vec[..., :quarter_len]
    back_part = half_vec[..., quarter_len:]
    return half_vec * jnp.cos(angles) + jnp.concatenate(
        [-back_part, front_part], axis=-1
    ) * jnp.sin(angles)


def apply_rotary(normed_heads, token_positions):
    half_point = normed_heads.shape[-1] // 2
    grid_row = token_positions // GRID_ROW_WIDTH
    grid_col = token_positions % GRID_ROW_WIDTH
    return jnp.concatenate(
        [
            turn_half(normed_heads[..., :half_point], grid_row),
            turn_half(normed_heads[..., half_point:], grid_col),
        ],
        axis=-1,
    )


def row_norm(rows_wide, gain_vec):
    inverse_rms = lax.rsqrt(jnp.mean(rows_wide * rows_wide, axis=-1, keepdims=True) + eps_norm)
    return (rows_wide * inverse_rms * gain_vec).astype(jnp.bfloat16)


def contract_units(left_rows, right_rows):
    return lax.dot_general(
        left_rows, right_rows, (((1,), (1,)), ((), ())), preferred_element_type=jnp.float32
    )


def shards(
    x_rows,
    queries,
    keys,
    values,
    query_norm_gain,
    key_norm_gain,
    out_weight,
    ffn_gain,
    gate_weight,
    value_weight,
    conv_gate,
    conv_value,
    down_weight,
):
    collected = (
        lax.all_gather(gate_weight, "sp", axis=0, tiled=True),
        lax.all_gather(value_weight, "sp", axis=0, tiled=True),
        lax.all_gather(down_weight, "sp", axis=0, tiled=True),
    )
    tokens_here = queries.shape[0]
    query_heads = queries.shape[1] // HEAD_SIZE
    key_heads = keys.shape[1] // HEAD_SIZE
    group_width = query_heads // key_heads
    lane_rows = group_width * tokens_here
    token_positions = lax.axis_index("sp") * tokens_here + jnp.arange(tokens_here, dtype=jnp.int32)
    rotated_queries = apply_rotary(
        per_head_norm(queries.reshape(tokens_here, query_heads, HEAD_SIZE), query_norm_gain),
        token_positions,
    )
    query_lanes = rotated_queries.reshape(tokens_here, key_heads, group_width, HEAD_SIZE).transpose(
        1, 2, 0, 3
    )
    query_lanes = query_lanes.reshape(key_heads, lane_rows, HEAD_SIZE) * HEAD_SIZE ** (-0.5)
    start_state = (
        jnp.full((key_heads, lane_rows), -1e30, jnp.float32),
        jnp.zeros((key_heads, lane_rows), jnp.float32),
        jnp.zeros((key_heads, lane_rows, HEAD_SIZE), jnp.float32),
    )
    key_piece = lax.all_gather(keys, "sp", axis=0, tiled=True)
    value_piece = lax.all_gather(values, "sp", axis=0, tiled=True)
    row_count = key_piece.shape[0]
    key_places = jnp.arange(row_count, dtype=jnp.int32)
    turned = apply_rotary(
        per_head_norm(key_piece.reshape(row_count, key_heads, HEAD_SIZE), key_norm_gain), key_places
    )
    key_span = math.gcd(row_count, 2048)
    span_count = row_count // key_span
    turned = turned.reshape(span_count, key_span, key_heads, HEAD_SIZE)
    value_matrix = value_piece.reshape(span_count, key_span, key_heads, HEAD_SIZE)

    def one_span(state_now, inputs):
        running_top, denominator, weighted = state_now
        key_block, value_block = inputs
        scores = jnp.einsum("hrd,shd->hrs", query_lanes, key_block, precision=lax.Precision.HIGHEST)
        new_top = jnp.maximum(running_top, jnp.max(scores, axis=-1))
        factor = jnp.exp(running_top - new_top)
        weights = jnp.exp(scores - new_top[..., None])
        denominator = denominator * factor + jnp.sum(weights, axis=-1)
        weighted = weighted * factor[..., None] + jnp.einsum(
            "hrs,shd->hrd",
            weights.astype(jnp.bfloat16),
            value_block,
            preferred_element_type=jnp.float32,
        )
        return ((new_top, denominator, weighted), None)

    folded_state, _ = lax.scan(one_span, start_state, (turned, value_matrix))
    running_top, denominator, weighted = folded_state
    attended = (weighted / denominator[..., None]).reshape(
        key_heads, group_width, tokens_here, HEAD_SIZE
    )
    attended = (
        attended.transpose(2, 0, 1, 3)
        .reshape(tokens_here, query_heads * HEAD_SIZE)
        .astype(jnp.bfloat16)
    )
    share_rows = tokens_here // lax.axis_size("tp")
    head_share = lax.psum_scatter(
        jnp.dot(attended, out_weight, preferred_element_type=jnp.float32).astype(jnp.bfloat16),
        "tp",
        scatter_dimension=0,
        tiled=True,
    ).astype(jnp.float32)
    own_rows = lax.dynamic_slice_in_dim(x_rows, lax.axis_index("tp") * share_rows, share_rows, 0)
    middle_rows = own_rows.astype(jnp.float32) + head_share
    normed = lax.all_gather(row_norm(middle_rows, ffn_gain), "tp", axis=0, tiled=True)
    unit_local = gate_weight.shape[1]
    gate_pre = jnp.dot(normed, collected[0], preferred_element_type=jnp.float32).astype(
        jnp.bfloat16
    )
    value_pre = jnp.dot(normed, collected[1], preferred_element_type=jnp.float32).astype(
        jnp.bfloat16
    )
    joined = jnp.concatenate([gate_pre, value_pre], axis=1)
    padded = with_halo(joined, (("sp", 0),), 1).astype(jnp.float32)
    conv_taps = jnp.concatenate([conv_gate, conv_value], axis=1)
    convolved = conv_taps[0] * padded[:-2] + conv_taps[1] * padded[1:-1] + conv_taps[2] * padded[2:]
    hidden = (jax.nn.silu(convolved[:, :unit_local]) * convolved[:, unit_local:]).astype(
        jnp.bfloat16
    )
    unit_share = lax.psum_scatter(
        contract_units(hidden, collected[2]).astype(jnp.bfloat16),
        "tp",
        scatter_dimension=0,
        tiled=True,
    ).astype(jnp.float32)
    finished = (middle_rows + unit_share).astype(jnp.bfloat16)
    return lax.all_gather(finished, "tp", axis=0, tiled=True)

LANES = 128
MESH = pl.DeviceIdType.MESH
BF = jnp.bfloat16
F32 = jnp.float32


def rem(a, b):
    return a % b if isinstance(a, int) else lax.rem(a, b)


def nt(left, right):
    return lax.dot_general(left, right, (((1,), (1,)), ((), ())), preferred_element_type=F32)


def layer_kernel(
    n, x_ref, q_ref, kv_ref, qg_ref, kg_ref, cos_ref, sin_ref, wo_ref, fg_ref, w_ref,
    cg_ref, cv_ref, out_ref,
    wo_buf, kvbuf, qbuf, kcat, qcat, att_s, attbuf, po_s, po_r, mid, allnorm, edge_s, edge_r, wrecv,
    pre_g, pre_v, part, ddbuf, own_sum, rs_s, rs_r, fin_s, fin_r,
    loc, kv_ss, kv_rs, q_ss, q_rs, w_ss, w_rs, wf_ss, wf_rs, dw_ss, dw_rs, df_ss, df_rs, o_ss, o_rs, po_sem, ag_ss, ag_rs, fw_ss, fw_rs,
    h_sem, dd_ss, dd_rs, c_ss, c_rs, fin_sem,
):
    sp = lax.axis_index("sp")
    core = lax.axis_index("tp")
    mate = 1 - core
    rows = x_ref.shape[0]
    half_rows = rows // 2
    width = x_ref.shape[1]
    kv_heads = kv_ref.shape[1] // LANES
    plane = n // 4
    group = 2 * plane
    tokens = n * rows
    q_tokens = kv_heads * rows
    units = w_ref.shape[1] // 3
    head_at = rem(sp, kv_heads)
    q_base = sp - head_at
    place = rem(sp, plane)
    side = rem(sp // plane, 2)
    wing = sp // (2 * plane)
    member = wing * plane + place

    def chip(m, at_side):
        return (m // plane) * (2 * plane) + at_side * plane + rem(m, plane)

    def ahead(d):
        return rem(wing + d // plane, 2) * plane + rem(place + rem(d, plane), plane)

    def behind(d):
        return rem(wing + d // plane, 2) * plane + rem(
            place + plane - rem(d, plane), plane
        )

    twin = chip(member, 1 - side)

    def remote(src, dst, ss, rs, device):
        return pltpu.make_async_remote_copy(
            src_ref=src, dst_ref=dst, send_sem=ss, recv_sem=rs, device_id=device, device_id_type=MESH
        )

    def lane_block(k):
        return pl.ds(pl.multiple_of(k * LANES, LANES), LANES)

    def span(start, size, unit):
        return pl.ds(pl.multiple_of(start, unit), size)

    def loop(lo, hi, fn):
        def step(k, carry):
            fn(k)
            return carry

        lax.fori_loop(lo, hi, step, 0)

    barrier = pltpu.get_barrier_semaphore()

    def greet(d):
        t = rem(sp + d, n)
        pl.semaphore_signal(barrier, inc=1, device_id=(t, core), device_id_type=MESH)

    loop(1, n, greet)
    pl.semaphore_signal(barrier, inc=1, device_id=(sp, mate), device_id_type=MESH)
    pl.semaphore_wait(barrier, n)

    def q_copy(d):
        t = q_base + rem(head_at + d, kv_heads)
        return remote(
            q_ref.at[:, lane_block(t - q_base)], qbuf.at[span(head_at * rows, rows, rows)],
            q_ss.at[d], q_rs.at[d], (t, core),
        )

    def kv_copy(d):
        t = rem(sp + d, n)
        return remote(
            kv_ref.at[:, lane_block(rem(t, kv_heads))], kvbuf.at[span(sp * rows, rows, rows)],
            kv_ss.at[d], kv_rs.at[d], (t, core),
        )

    up_part, down_part = slice(0, 2 * units), slice(2 * units, 3 * units)

    def w_copy(d, part_at, ss, rs):
        m = ahead(d)
        return remote(
            w_ref.at[m, part_at], wrecv.at[part_at, lane_block(sp)],
            ss.at[d], rs.at[d], (chip(m, side), core),
        )

    def twin_first(part_at, ss, rs):
        return remote(
            w_ref.at[member, part_at], wrecv.at[part_at, lane_block(sp)],
            ss.at[0], rs.at[0], (twin, core),
        )

    def twin_copy(d, part_at, ss, rs):
        at = wrecv.at[part_at, lane_block(chip(behind(d), side))]
        return remote(at, at, ss.at[d], rs.at[d], (twin, core))

    def pass_on(d, part_at, ss, rs, next_ss, next_rs):
        dst = wrecv.at[part_at, lane_block(chip(behind(d), side))]
        remote(dst, dst, ss.at[d], rs.at[d], (twin, core)).wait_recv()
        twin_copy(d, part_at, next_ss, next_rs).start()

    def twin_wait(d, part_at, ss, rs):
        dst = wrecv.at[part_at, lane_block(chip(behind(d), 1 - side))]
        remote(dst, dst, ss.at[d], rs.at[d], (twin, core)).wait_recv()

    later = plane + plane // 2
    gate_sems, gate_next = (w_ss, w_rs), (wf_ss, wf_rs)
    down_sems, down_next = (dw_ss, dw_rs), (df_ss, df_rs)

    own_q = pltpu.make_async_copy(
        q_ref.at[:, lane_block(head_at)], qbuf.at[span(head_at * rows, rows, rows)], loc.at[0]
    )
    own_kv = pltpu.make_async_copy(
        kv_ref.at[:, lane_block(head_at)], kvbuf.at[span(sp * rows, rows, rows)], loc.at[1]
    )
    own_w = pltpu.make_async_copy(w_ref.at[member], wrecv.at[:, lane_block(sp)], loc.at[2])
    own_q.start()
    wo_copy = pltpu.make_async_copy(wo_ref, wo_buf, loc.at[3])
    wo_copy.start()
    own_kv.start()
    loop(1, kv_heads, lambda d: q_copy(d).start())
    loop(1, n, lambda d: kv_copy(d).start())
    loop(1, plane, lambda d: w_copy(d, up_part, *gate_sems).start())
    own_w.start()

    lane = lax.broadcasted_iota(jnp.int32, (GRID_ROW_WIDTH, LANES), 1)
    low = lane < HEAD_SIZE
    first = rem(lane, 2 * HEAD_SIZE // 4) < HEAD_SIZE // 4
    by_row = rem(lane, HEAD_SIZE) < HEAD_SIZE // 2

    def turn(vals, grid_row):
        cos = jnp.where(by_row, cos_ref[pl.ds(grid_row, 1), :], cos_ref[:GRID_ROW_WIDTH, :])
        sin = jnp.where(by_row, sin_ref[pl.ds(grid_row, 1), :], sin_ref[:GRID_ROW_WIDTH, :])
        quarter = HEAD_SIZE // 4
        swapped = jnp.where(
            first, pltpu.roll(vals, LANES - quarter, 1), pltpu.roll(vals, quarter, 1)
        )
        return vals * cos + swapped * sin

    q_gain = jnp.concatenate([qg_ref[...]] * 2, axis=1)
    k_gain = jnp.concatenate([kg_ref[...]] * 2, axis=1)

    def split(vals):
        top = vals.astype(BF).astype(F32)
        return top, (vals - top).astype(BF).astype(F32)

    def make_q(r):
        at = span(r * GRID_ROW_WIDTH, GRID_ROW_WIDTH, GRID_ROW_WIDTH)
        vals = qbuf[at, :].astype(F32)
        sq = vals * vals
        low_sum = jnp.sum(jnp.where(low, sq, 0.0), axis=1, keepdims=True)
        high_sum = jnp.sum(jnp.where(low, 0.0, sq), axis=1, keepdims=True)
        inverse = jnp.where(
            low,
            lax.rsqrt(low_sum * (1.0 / HEAD_SIZE) + eps_norm),
            lax.rsqrt(high_sum * (1.0 / HEAD_SIZE) + eps_norm),
        )
        turned = turn(vals * inverse * q_gain, q_base * (rows // GRID_ROW_WIDTH) + r)
        top, rest = split(turned * HEAD_SIZE ** (-0.5))
        qcat[at, :] = jnp.where(low, top, pltpu.roll(rest, HEAD_SIZE, 1)).astype(BF)
        later = span(q_tokens + r * GRID_ROW_WIDTH, GRID_ROW_WIDTH, GRID_ROW_WIDTH)
        qcat[later, :] = jnp.where(low, pltpu.roll(top, HEAD_SIZE, 1), rest).astype(BF)

    own_q.wait()

    def q_take(d):
        s = rem(head_at + kv_heads - d, kv_heads)
        dst = qbuf.at[span(s * rows, rows, rows)]

        @pl.when(d > 0)
        def _():
            remote(dst, dst, q_ss.at[d], q_rs.at[d], (q_base + s, core)).wait_recv()

        for r in range(rows // GRID_ROW_WIDTH):
            make_q(s * (rows // GRID_ROW_WIDTH) + r)

    loop(0, kv_heads, q_take)
    twin_first(up_part, *gate_next).start()
    loop(plane, later, lambda d: w_copy(d, up_part, *gate_sems).start())
    steps = rows // GRID_ROW_WIDTH

    def make_k(r):
        at = span(r * GRID_ROW_WIDTH, GRID_ROW_WIDTH, GRID_ROW_WIDTH)
        vals = kvbuf[at, :].astype(F32)
        total = jnp.sum(jnp.where(low, vals * vals, 0.0), axis=1, keepdims=True)
        turned = turn(
            vals * lax.rsqrt(total * (1.0 / HEAD_SIZE) + eps_norm) * k_gain, r
        )
        top, rest = split(turned)
        kcat[at, :LANES] = jnp.where(low, top, pltpu.roll(top, HEAD_SIZE, 1)).astype(BF)
        kcat[at, LANES:] = jnp.where(low, rest, pltpu.roll(rest, HEAD_SIZE, 1)).astype(BF)

    own_kv.wait()

    def kv_take(d):
        s = rem(sp + n - d, n)
        dst = kvbuf.at[span(s * rows, rows, rows)]

        @pl.when(d > 0)
        def _():
            remote(dst, dst, kv_ss.at[d], kv_rs.at[d], (s, core)).wait_recv()

        for r in range(steps):
            make_k(s * steps + r)

    loop(0, n, kv_take)
    loop(1, plane, lambda d: pass_on(d, up_part, *gate_sems, *gate_next))

    def o_copy(d):
        k = rem(head_at + d, kv_heads)
        return remote(
            att_s.at[span(k * rows, rows, rows)], attbuf.at[:, lane_block(head_at)],
            o_ss.at[d], o_rs.at[d], (q_base + k, core),
        )

    low_rows = lax.broadcasted_iota(jnp.int32, (rows, LANES), 1) < HEAD_SIZE

    def attend(k):
        both = jnp.concatenate(
            [qcat[span(k * rows, rows, rows), :], qcat[span(q_tokens + k * rows, rows, rows), :]],
            axis=0,
        )
        scores = nt(jnp.concatenate([both, both], axis=1), kcat[...])
        shifted = jnp.exp(scores - jnp.max(scores, axis=1, keepdims=True))
        total = jnp.sum(shifted, axis=1, keepdims=True)
        summed = jnp.dot(shifted.astype(BF), kvbuf[...], preferred_element_type=F32) / total
        return jnp.where(
            low_rows, pltpu.roll(summed[:rows], HEAD_SIZE, 1), summed[rows:]
        ).astype(BF)

    def attend_send(d):
        k = rem(head_at + d, kv_heads)
        att_s[span(k * rows, rows, rows), :] = attend(k)

        @pl.when(d < kv_heads)
        def _():
            o_copy(d).start()

    loop(1, kv_heads + 1, attend_send)
    attbuf[:, lane_block(head_at)] = att_s[span(head_at * rows, rows, rows), :]

    def o_wait(d):
        s = rem(head_at + kv_heads - d, kv_heads)
        dst = attbuf.at[:, lane_block(s)]
        remote(dst, dst, o_ss.at[d], o_rs.at[d], (q_base + s, core)).wait_recv()

    loop(1, kv_heads, o_wait)

    wo_copy.wait()
    po_s[...] = jnp.dot(attbuf[...], wo_buf[...], preferred_element_type=F32).astype(BF)
    po_copy = remote(
        po_s.at[span(mate * half_rows, half_rows, half_rows)], po_r, po_sem.at[0], po_sem.at[1],
        (sp, mate),
    )
    po_copy.start()
    mine = span(core * half_rows, half_rows, half_rows)
    base = x_ref[mine, :].astype(F32) + po_s[mine, :].astype(F32)
    po_copy.wait_recv()
    middle = base + po_r[...].astype(F32)
    mid[...] = middle
    scaled = lax.rsqrt(jnp.mean(middle * middle, axis=1, keepdims=True) + eps_norm)
    normed = (middle * scaled * fg_ref[...]).astype(BF)

    def slot(k, c):
        return allnorm.at[span(k * rows + c * half_rows, half_rows, half_rows)]

    allnorm[span(member * rows + core * half_rows, half_rows, half_rows), :] = normed

    def ag_copy(d):
        to = ahead(rem(d, plane)) if d != plane else ahead(d)
        of = member if d <= plane else (1 - wing) * plane + place
        return remote(
            slot(of, core), slot(of, core), ag_ss.at[d], ag_rs.at[d], (chip(to, side), core)
        )

    def fw_copy(d):
        s = behind(d)
        return remote(slot(s, core), slot(s, core), fw_ss.at[d], fw_rs.at[d], (sp, mate))

    def ag_wait(d):
        s = behind(d)
        remote(slot(s, core), slot(s, core), ag_ss.at[d], ag_rs.at[d], (sp, mate)).wait_recv()
        fw_copy(d).start()

    ag_copy(plane).start()
    for d in range(1, plane):
        ag_copy(d).start()
    fw_copy(0).start()

    own_w.wait()
    loop(later, group, lambda d: w_copy(d, up_part, *gate_sems).start())
    loop(plane, later, lambda d: pass_on(d, up_part, *gate_sems, *gate_next))
    ag_wait(plane)
    for d in range(plane + 1, group):
        ag_copy(d).start()
    loop(plane, group, lambda d: w_copy(d, down_part, *down_sems).start())
    loop(1, plane, lambda d: w_copy(d, down_part, *down_sems).start())
    loop(later, group, lambda d: pass_on(d, up_part, *gate_sems, *gate_next))
    twin_first(down_part, *down_next).start()

    def up(block):
        both = nt(block, wrecv[: 2 * units, :]).astype(BF).astype(F32)
        return both[:, :units], both[:, units:]

    seg = plane * rows
    pitch = seg + 16

    def row_of(m):
        return (m // plane) * pitch + rem(m, plane) * rows

    def take(d):
        @pl.when(jnp.logical_and(d > 0, d != plane))
        def _():
            ag_wait(d)

    def mate_wait(d):
        s = behind(d)
        remote(slot(s, mate), slot(s, mate), fw_ss.at[d], fw_rs.at[d], (sp, mate)).wait_recv()

    def up_rows(k):
        side_at = rem(wing + k, 2)
        loop(k * plane, (k + 1) * plane, mate_wait)
        gate, value = up(allnorm[span(side_at * seg, seg, rows), :])
        at = span(side_at * pitch + 8, seg, 8)
        pre_g[at, :] = gate
        pre_v[at, :] = value

    loop(0, group, take)
    loop(0, group, lambda d: twin_wait(d, up_part, *gate_next))
    loop(0, 2, up_rows)
    loop(1, group, lambda d: pass_on(d, down_part, *down_sems, *down_next))

    edge_at = (8, 8 + seg - 1, pitch + 8, pitch + 8 + seg - 1)
    edge_s[...] = jnp.concatenate(
        [
            jnp.concatenate([pre[k : k + 1, :] for k in edge_at] * 2, axis=0)
            for pre in (pre_g, pre_v)
        ],
        axis=0,
    )
    edge_copy = remote(edge_s, edge_r, h_sem.at[0], h_sem.at[1], (twin, core))
    edge_copy.start()
    loop(0, group, lambda d: twin_wait(d, down_part, *down_next))
    edge_copy.wait_recv()
    for pre, first_row in ((pre_g, 0), (pre_v, 8)):
        near = [
            jnp.broadcast_to(edge_r[first_row + k : first_row + k + 1, :], (8, units))
            for k in range(4)
        ]
        none = jnp.zeros((8, units), F32)
        pre[0:8, :] = jnp.where(side == 0, none, near[1])
        pre[8 + seg : pitch, :] = jnp.where(side == 0, near[0], near[2])
        pre[pitch : pitch + 8, :] = jnp.where(side == 0, near[1], near[3])
        pre[pitch + 8 + seg :, :] = jnp.where(side == 0, near[2], none)

    def convolve(ref, taps, k):
        block = ref[span(row_of(k), rows + 16, 8), :]
        return (
            taps[0:1, :] * block[7 : 7 + rows]
            + taps[1:2, :] * block[8 : 8 + rows]
            + taps[2:3, :] * block[9 : 9 + rows]
        )

    def dd_copy(d):
        return remote(
            part.at[d, span(mate * half_rows, half_rows, half_rows)], ddbuf.at[d],
            dd_ss.at[d], dd_rs.at[d], (sp, mate),
        )

    def c_copy(d, to):
        return remote(rs_s.at[d], rs_r.at[d], c_ss.at[d], c_rs.at[d], (chip(to, side), core))

    def c_near(d):
        return c_copy(d, ahead(rem(d, plane)))

    def combine(d):
        dd_copy(d).wait_recv()
        return part[d, mine, :].astype(F32) + ddbuf[d].astype(F32)

    def send_sum(d):
        rs_s[d] = combine(d).astype(BF)
        c_near(d).start()

    def order(j):
        return plane * (1 - j // plane) + rem(j + 1, plane)

    def down(j):
        d = order(j)
        k = ahead(d)
        gate = convolve(pre_g, cg_ref, k)
        value = convolve(pre_v, cv_ref, k)
        hidden = (gate / (1.0 + jnp.exp(-gate)) * value).astype(BF)
        part[d] = jnp.dot(hidden, wrecv[2 * units :, :], preferred_element_type=F32).astype(BF)
        dd_copy(d).start()
        last = order(jnp.maximum(j - 1, 0))

        @pl.when(jnp.logical_and(j > 0, rem(last, plane) > 0))
        def _():
            send_sum(last)

    loop(0, group, down)

    def add_in(d):
        remote(rs_r.at[d], rs_r.at[d], c_ss.at[d], c_rs.at[d], (sp, mate)).wait_recv()
        own_sum[...] = own_sum[...] + rs_r[d].astype(F32)

    own_sum[...] = combine(plane)
    loop(plane + 1, group, add_in)
    rs_s[plane] = own_sum[...].astype(BF)
    far_copy = c_copy(plane, (1 - wing) * plane + place)
    far_copy.start()
    own_sum[...] = mid[...] + combine(0)
    loop(1, plane + 1, add_in)
    fin_s[...] = own_sum[...].astype(BF)
    fin_copy = remote(fin_s, fin_r, fin_sem.at[0], fin_sem.at[1], (sp, mate))
    fin_copy.start()
    out_ref[mine, :] = fin_s[...]

    loop(1, kv_heads, lambda d: q_copy(d).wait_send())
    loop(1, n, lambda d: kv_copy(d).wait_send())
    loop(1, group, lambda d: w_copy(d, up_part, *gate_sems).wait_send())
    loop(1, group, lambda d: w_copy(d, down_part, *down_sems).wait_send())
    loop(0, group, lambda d: twin_copy(d, up_part, *gate_next).wait_send())
    loop(0, group, lambda d: twin_copy(d, down_part, *down_next).wait_send())
    loop(1, kv_heads, lambda d: o_copy(d).wait_send())
    po_copy.wait_send()
    for d in range(1, group):
        ag_copy(d).wait_send()
    loop(0, group, lambda d: fw_copy(d).wait_send())
    edge_copy.wait_send()
    loop(0, group, lambda d: dd_copy(d).wait_send())
    loop(1, plane, lambda d: c_near(d).wait_send())
    loop(plane + 1, group, lambda d: c_near(d).wait_send())
    far_copy.wait_send()
    fin_copy.wait_send()
    fin_copy.wait_recv()
    out_ref[span(mate * half_rows, half_rows, half_rows), :] = fin_r[...]


def rotary_tables(count):
    lanes = jnp.arange(LANES)
    length = HEAD_SIZE // 2
    rate_at = (lanes % (length // 2)).astype(F32)
    rates = 1.0 / theta ** (rate_at * 2.0 / length)
    angles = jnp.arange(count, dtype=F32)[:, None] * rates[None, :]
    sign = jnp.where(lanes % length < length // 2, -1.0, 1.0)
    return jnp.cos(angles), jnp.sin(angles) * sign[None, :]


def kernel_shards(
    n, x_rows, queries, keys, values, query_norm_gain, key_norm_gain, out_weight, ffn_gain,
    gate_weight, value_weight, conv_gate, conv_value, down_weight,
):
    rows, width = x_rows.shape
    kv_heads = keys.shape[1] // HEAD_SIZE
    plane = n // 4
    group = 2 * plane
    unit_local = gate_weight.shape[1]
    units = unit_local // group
    depth = gate_weight.shape[0]
    kv = jnp.concatenate(
        [keys.reshape(rows, kv_heads, HEAD_SIZE), values.reshape(rows, kv_heads, HEAD_SIZE)], axis=-1
    ).reshape(rows, kv_heads * LANES)
    turned = [
        w.T.reshape(group, units, depth) for w in (gate_weight, value_weight, down_weight)
    ]
    weights = jnp.concatenate(turned, axis=1)
    at = lax.axis_index("sp")
    chip = (at // group) * plane + rem(at, plane)
    taps = [lax.dynamic_slice_in_dim(t, chip * units, units, 1) for t in (conv_gate, conv_value)]
    cos, sin = rotary_tables(max(GRID_ROW_WIDTH, n * rows // GRID_ROW_WIDTH))
    tokens, q_tokens, span_rows = n * rows, kv_heads * rows, group * rows
    half_rows = rows // 2
    dma = pltpu.SemaphoreType.DMA
    vm = pltpu.VMEM
    scratch = [
        vm(out_weight.shape, BF), vm((tokens, LANES), BF), vm((q_tokens, LANES), BF), vm((tokens, 2 * LANES), BF),
        vm((2 * q_tokens, LANES), BF), vm((q_tokens, LANES), BF), vm((rows, kv_heads * LANES), BF),
        vm((rows, width), BF), vm((half_rows, width), BF), vm((half_rows, width), F32),
        vm((span_rows, width), BF), vm((16, units), F32),
        vm((16, units), F32), vm((3 * units, width), BF),
        vm((span_rows + 32, units), F32), vm((span_rows + 32, units), F32),
        vm((group, rows, width), BF), vm((group, half_rows, width), BF),
        vm((half_rows, width), F32), vm((group, half_rows, width), BF),
        vm((group, half_rows, width), BF), vm((half_rows, width), BF), vm((half_rows, width), BF),
        dma((4,)), dma((n,)), dma((n,)), dma((kv_heads,)), dma((kv_heads,)), *[dma((group,))] * 8,
        dma((kv_heads,)), dma((kv_heads,)), dma((2,)), dma((group,)), dma((group,)),
        dma((group,)), dma((group,)), dma((2,)), dma((group,)), dma((group,)),
        dma((group,)), dma((group,)), dma((2,)),
    ]
    args = (
        x_rows, queries, kv, query_norm_gain[None, :], key_norm_gain[None, :],
        cos, sin, out_weight, ffn_gain[None, :], weights, taps[0], taps[1],
    )
    return pl.pallas_call(
        lambda *refs: layer_kernel(n, *refs),
        out_shape=jax.ShapeDtypeStruct((rows, width), BF),
        in_specs=[
            pl.BlockSpec(memory_space=pl.ANY if a is out_weight else pltpu.VMEM) for a in args
        ],
        out_specs=pl.BlockSpec(memory_space=pltpu.VMEM),
        scratch_shapes=scratch,
        compiler_params=pltpu.CompilerParams(
            collective_id=0, has_side_effects=True, vmem_limit_bytes=60 * 2**20
        ),
        name="layer",
    )(*args)


def suits(mesh, sizes):
    n, pair = mesh.shape["sp"], mesh.shape["tp"]
    x_rows, queries, keys, gate = sizes
    if pair != 2 or n % 4:
        return False
    rows, group = x_rows[0] // n, n // 2
    heads = keys[1] // pair // HEAD_SIZE
    units = gate[1] // pair
    return (
        rows % GRID_ROW_WIDTH == 0
        and rows % 32 == 0
        and queries[1] == 2 * keys[1]
        and n % heads == 0
        and 2 * HEAD_SIZE == LANES
        and x_rows[1] == n * LANES
        and units % (16 * group) == 0
    )


def solution(mesh):
    placed = (
        P("sp", None),
        P("sp", "tp"),
        P("sp", "tp"),
        P("sp", "tp"),
        P(),
        P(),
        P("tp", None),
        P(),
        P("sp", "tp"),
        P("sp", "tp"),
        P(None, "tp"),
        P(None, "tp"),
        P("sp", "tp"),
    )
    def run(*arrays):
        n = mesh.shape["sp"]
        fits = suits(mesh, [arrays[k].shape for k in (0, 1, 2, 8)])
        local = functools.partial(kernel_shards, n) if fits else shards
        return jax.shard_map(
            local, mesh=mesh, in_specs=placed, out_specs=P("sp", None), check_vma=False
        )(*arrays)

    return run
```

```python
import functools
import math

import jax
import jax.numpy as jnp
from jax import lax
from jax.experimental import pallas as pl
from jax.experimental.pallas import tpu as pltpu
from jax.sharding import PartitionSpec as P

HEAD_SIZE = 64
GRID_ROW_WIDTH = 64


eps_norm = 1e-06
theta = 10000.0


def with_halo(cells, sides, width):
    for axis, dim in sides:
        count = lax.axis_size(axis)
        ends = count - 1
        head = lax.slice_in_dim(cells, 0, width, axis=dim)
        tail = lax.slice_in_dim(cells, cells.shape[dim] - width, cells.shape[dim], axis=dim)
        cells = jnp.concatenate(
            [
                lax.ppermute(tail, axis, [(i, (i + 1) % count) for i in range(ends)]),
                cells,
                lax.ppermute(head, axis, [((i + 1) % count, i) for i in range(ends)]),
            ],
            axis=dim,
        )
    return cells


def per_head_norm(head_block, gain_vec):
    wide_vals = head_block.astype(jnp.float32)
    inverse_rms = lax.rsqrt(jnp.mean(wide_vals * wide_vals, axis=-1, keepdims=True) + eps_norm)
    return wide_vals * inverse_rms * gain_vec


def turn_half(half_vec, places):
    quarter_len = half_vec.shape[-1] // 2
    inverse_rates = 1.0 / theta ** (
        jnp.arange(quarter_len, dtype=jnp.float32) * 2.0 / half_vec.shape[-1]
    )
    angles = places.astype(jnp.float32)[:, None] * inverse_rates[None, :]
    angles = jnp.concatenate([angles, angles], axis=-1)[:, None, :]
    front_part = half_vec[..., :quarter_len]
    back_part = half_vec[..., quarter_len:]
    return half_vec * jnp.cos(angles) + jnp.concatenate(
        [-back_part, front_part], axis=-1
    ) * jnp.sin(angles)


def apply_rotary(normed_heads, token_positions):
    half_point = normed_heads.shape[-1] // 2
    grid_row = token_positions // GRID_ROW_WIDTH
    grid_col = token_positions % GRID_ROW_WIDTH
    return jnp.concatenate(
        [
            turn_half(normed_heads[..., :half_point], grid_row),
            turn_half(normed_heads[..., half_point:], grid_col),
        ],
        axis=-1,
    )


def row_norm(rows_wide, gain_vec):
    inverse_rms = lax.rsqrt(jnp.mean(rows_wide * rows_wide, axis=-1, keepdims=True) + eps_norm)
    return (rows_wide * inverse_rms * gain_vec).astype(jnp.bfloat16)


def contract_units(left_rows, right_rows):
    return lax.dot_general(
        left_rows, right_rows, (((1,), (1,)), ((), ())), preferred_element_type=jnp.float32
    )


def shards(
    x_rows,
    queries,
    keys,
    values,
    query_norm_gain,
    key_norm_gain,
    out_weight,
    ffn_gain,
    gate_weight,
    value_weight,
    conv_gate,
    conv_value,
    down_weight,
):
    collected = (
        lax.all_gather(gate_weight, "sp", axis=0, tiled=True),
        lax.all_gather(value_weight, "sp", axis=0, tiled=True),
        lax.all_gather(down_weight, "sp", axis=0, tiled=True),
    )
    tokens_here = queries.shape[0]
    query_heads = queries.shape[1] // HEAD_SIZE
    key_heads = keys.shape[1] // HEAD_SIZE
    group_width = query_heads // key_heads
    lane_rows = group_width * tokens_here
    token_positions = lax.axis_index("sp") * tokens_here + jnp.arange(tokens_here, dtype=jnp.int32)
    rotated_queries = apply_rotary(
        per_head_norm(queries.reshape(tokens_here, query_heads, HEAD_SIZE), query_norm_gain),
        token_positions,
    )
    query_lanes = rotated_queries.reshape(tokens_here, key_heads, group_width, HEAD_SIZE).transpose(
        1, 2, 0, 3
    )
    query_lanes = query_lanes.reshape(key_heads, lane_rows, HEAD_SIZE) * HEAD_SIZE ** (-0.5)
    start_state = (
        jnp.full((key_heads, lane_rows), -1e30, jnp.float32),
        jnp.zeros((key_heads, lane_rows), jnp.float32),
        jnp.zeros((key_heads, lane_rows, HEAD_SIZE), jnp.float32),
    )
    key_piece = lax.all_gather(keys, "sp", axis=0, tiled=True)
    value_piece = lax.all_gather(values, "sp", axis=0, tiled=True)
    row_count = key_piece.shape[0]
    key_places = jnp.arange(row_count, dtype=jnp.int32)
    turned = apply_rotary(
        per_head_norm(key_piece.reshape(row_count, key_heads, HEAD_SIZE), key_norm_gain), key_places
    )
    key_span = math.gcd(row_count, 2048)
    span_count = row_count // key_span
    turned = turned.reshape(span_count, key_span, key_heads, HEAD_SIZE)
    value_matrix = value_piece.reshape(span_count, key_span, key_heads, HEAD_SIZE)

    def one_span(state_now, inputs):
        running_top, denominator, weighted = state_now
        key_block, value_block = inputs
        scores = jnp.einsum("hrd,shd->hrs", query_lanes, key_block, precision=lax.Precision.HIGHEST)
        new_top = jnp.maximum(running_top, jnp.max(scores, axis=-1))
        factor = jnp.exp(running_top - new_top)
        weights = jnp.exp(scores - new_top[..., None])
        denominator = denominator * factor + jnp.sum(weights, axis=-1)
        weighted = weighted * factor[..., None] + jnp.einsum(
            "hrs,shd->hrd",
            weights.astype(jnp.bfloat16),
            value_block,
            preferred_element_type=jnp.float32,
        )
        return ((new_top, denominator, weighted), None)

    folded_state, _ = lax.scan(one_span, start_state, (turned, value_matrix))
    running_top, denominator, weighted = folded_state
    attended = (weighted / denominator[..., None]).reshape(
        key_heads, group_width, tokens_here, HEAD_SIZE
    )
    attended = (
        attended.transpose(2, 0, 1, 3)
        .reshape(tokens_here, query_heads * HEAD_SIZE)
        .astype(jnp.bfloat16)
    )
    share_rows = tokens_here // lax.axis_size("tp")
    head_share = lax.psum_scatter(
        jnp.dot(attended, out_weight, preferred_element_type=jnp.float32).astype(jnp.bfloat16),
        "tp",
        scatter_dimension=0,
        tiled=True,
    ).astype(jnp.float32)
    own_rows = lax.dynamic_slice_in_dim(x_rows, lax.axis_index("tp") * share_rows, share_rows, 0)
    middle_rows = own_rows.astype(jnp.float32) + head_share
    normed = lax.all_gather(row_norm(middle_rows, ffn_gain), "tp", axis=0, tiled=True)
    unit_local = gate_weight.shape[1]
    gate_pre = jnp.dot(normed, collected[0], preferred_element_type=jnp.float32).astype(
        jnp.bfloat16
    )
    value_pre = jnp.dot(normed, collected[1], preferred_element_type=jnp.float32).astype(
        jnp.bfloat16
    )
    joined = jnp.concatenate([gate_pre, value_pre], axis=1)
    padded = with_halo(joined, (("sp", 0),), 1).astype(jnp.float32)
    conv_taps = jnp.concatenate([conv_gate, conv_value], axis=1)
    convolved = conv_taps[0] * padded[:-2] + conv_taps[1] * padded[1:-1] + conv_taps[2] * padded[2:]
    hidden = (jax.nn.silu(convolved[:, :unit_local]) * convolved[:, unit_local:]).astype(
        jnp.bfloat16
    )
    unit_share = lax.psum_scatter(
        contract_units(hidden, collected[2]).astype(jnp.bfloat16),
        "tp",
        scatter_dimension=0,
        tiled=True,
    ).astype(jnp.float32)
    finished = (middle_rows + unit_share).astype(jnp.bfloat16)
    return lax.all_gather(finished, "tp", axis=0, tiled=True)

LANES = 128
MESH = pl.DeviceIdType.MESH
BF = jnp.bfloat16
F32 = jnp.float32


def rem(a, b):
    return a % b if isinstance(a, int) else lax.rem(a, b)


def nt(left, right):
    return lax.dot_general(left, right, (((1,), (1,)), ((), ())), preferred_element_type=F32)


def layer_kernel(
    n, x_ref, q_ref, kv_ref, qg_ref, kg_ref, cos_ref, sin_ref, wo_ref, fg_ref, w_ref,
    cg_ref, cv_ref, out_ref,
    wo_buf, kvbuf, qbuf, kcat, qcat, att_s, attbuf, po_s, po_r, mid, allnorm, edge_s, edge_r, wrecv,
    pre_g, pre_v, part, ddbuf, own_sum, rs_s, rs_r, fin_s, fin_r,
    loc, kv_ss, kv_rs, q_ss, q_rs, w_ss, w_rs, wf_ss, wf_rs, dw_ss, dw_rs, df_ss, df_rs, o_ss, o_rs, po_sem, ag_ss, ag_rs, fw_ss, fw_rs,
    ch_ss, ch_rs, h_sem, dd_ss, dd_rs, c_ss, c_rs, fin_sem,
):
    sp = lax.axis_index("sp")
    core = lax.axis_index("tp")
    mate = 1 - core
    rows = x_ref.shape[0]
    half_rows = rows // 2
    width = x_ref.shape[1]
    kv_heads = kv_ref.shape[1] // LANES
    plane = n // 4
    group = 2 * plane
    tokens = n * rows
    q_tokens = kv_heads * rows
    units = w_ref.shape[1] // 3
    head_at = rem(sp, kv_heads)
    q_base = sp - head_at
    place = rem(sp, plane)
    side = rem(sp // plane, 2)
    wing = sp // (2 * plane)
    member = wing * plane + place

    def chip(m, at_side):
        return (m // plane) * (2 * plane) + at_side * plane + rem(m, plane)

    def ahead(d):
        return rem(wing + d // plane, 2) * plane + rem(place + rem(d, plane), plane)

    def behind(d):
        return rem(wing + d // plane, 2) * plane + rem(
            place + plane - rem(d, plane), plane
        )

    twin = chip(member, 1 - side)

    def remote(src, dst, ss, rs, device):
        return pltpu.make_async_remote_copy(
            src_ref=src, dst_ref=dst, send_sem=ss, recv_sem=rs, device_id=device, device_id_type=MESH
        )

    def lane_block(k):
        return pl.ds(pl.multiple_of(k * LANES, LANES), LANES)

    def span(start, size, unit):
        return pl.ds(pl.multiple_of(start, unit), size)

    def loop(lo, hi, fn):
        def step(k, carry):
            fn(k)
            return carry

        lax.fori_loop(lo, hi, step, 0)

    barrier = pltpu.get_barrier_semaphore()

    def greet(d):
        t = rem(sp + d, n)
        pl.semaphore_signal(barrier, inc=1, device_id=(t, core), device_id_type=MESH)

    loop(1, n, greet)
    pl.semaphore_signal(barrier, inc=1, device_id=(sp, mate), device_id_type=MESH)
    pl.semaphore_wait(barrier, n)

    def q_copy(d):
        t = q_base + rem(head_at + d, kv_heads)
        return remote(
            q_ref.at[:, lane_block(t - q_base)], qbuf.at[span(head_at * rows, rows, rows)],
            q_ss.at[d], q_rs.at[d], (t, core),
        )

    def kv_copy(d):
        t = rem(sp + d, n)
        return remote(
            kv_ref.at[:, lane_block(rem(t, kv_heads))], kvbuf.at[span(sp * rows, rows, rows)],
            kv_ss.at[d], kv_rs.at[d], (t, core),
        )

    up_part, down_part = slice(0, 2 * units), slice(2 * units, 3 * units)

    def w_copy(d, part_at, ss, rs):
        m = ahead(d)
        return remote(
            w_ref.at[m, part_at], wrecv.at[part_at, lane_block(sp)],
            ss.at[d], rs.at[d], (chip(m, side), core),
        )

    def twin_first(part_at, ss, rs):
        return remote(
            w_ref.at[member, part_at], wrecv.at[part_at, lane_block(sp)],
            ss.at[0], rs.at[0], (twin, core),
        )

    def twin_copy(d, part_at, ss, rs):
        at = wrecv.at[part_at, lane_block(chip(behind(d), side))]
        return remote(at, at, ss.at[d], rs.at[d], (twin, core))

    def pass_on(d, part_at, ss, rs, next_ss, next_rs):
        dst = wrecv.at[part_at, lane_block(chip(behind(d), side))]
        remote(dst, dst, ss.at[d], rs.at[d], (twin, core)).wait_recv()
        twin_copy(d, part_at, next_ss, next_rs).start()

    def twin_wait(d, part_at, ss, rs):
        dst = wrecv.at[part_at, lane_block(chip(behind(d), 1 - side))]
        remote(dst, dst, ss.at[d], rs.at[d], (twin, core)).wait_recv()

    later = plane + plane // 2
    gate_sems, gate_next = (w_ss, w_rs), (wf_ss, wf_rs)
    down_sems, down_next = (dw_ss, dw_rs), (df_ss, df_rs)

    own_q = pltpu.make_async_copy(
        q_ref.at[:, lane_block(head_at)], qbuf.at[span(head_at * rows, rows, rows)], loc.at[0]
    )
    own_kv = pltpu.make_async_copy(
        kv_ref.at[:, lane_block(head_at)], kvbuf.at[span(sp * rows, rows, rows)], loc.at[1]
    )
    own_w = pltpu.make_async_copy(w_ref.at[member], wrecv.at[:, lane_block(sp)], loc.at[2])
    own_q.start()
    wo_copy = pltpu.make_async_copy(wo_ref, wo_buf, loc.at[3])
    wo_copy.start()
    own_kv.start()
    loop(1, kv_heads, lambda d: q_copy(d).start())
    loop(1, n, lambda d: kv_copy(d).start())
    loop(1, plane, lambda d: w_copy(d, up_part, *gate_sems).start())
    loop(1, plane, lambda d: w_copy(d, down_part, *down_sems).start())
    own_w.start()

    lane = lax.broadcasted_iota(jnp.int32, (GRID_ROW_WIDTH, LANES), 1)
    low = lane < HEAD_SIZE
    first = rem(lane, 2 * HEAD_SIZE // 4) < HEAD_SIZE // 4
    by_row = rem(lane, HEAD_SIZE) < HEAD_SIZE // 2

    def turn(vals, grid_row):
        cos = jnp.where(by_row, cos_ref[pl.ds(grid_row, 1), :], cos_ref[:GRID_ROW_WIDTH, :])
        sin = jnp.where(by_row, sin_ref[pl.ds(grid_row, 1), :], sin_ref[:GRID_ROW_WIDTH, :])
        quarter = HEAD_SIZE // 4
        swapped = jnp.where(
            first, pltpu.roll(vals, LANES - quarter, 1), pltpu.roll(vals, quarter, 1)
        )
        return vals * cos + swapped * sin

    q_gain = jnp.concatenate([qg_ref[...]] * 2, axis=1)
    k_gain = jnp.concatenate([kg_ref[...]] * 2, axis=1)

    def split(vals):
        top = vals.astype(BF).astype(F32)
        return top, (vals - top).astype(BF).astype(F32)

    def make_q(r):
        at = span(r * GRID_ROW_WIDTH, GRID_ROW_WIDTH, GRID_ROW_WIDTH)
        vals = qbuf[at, :].astype(F32)
        sq = vals * vals
        low_sum = jnp.sum(jnp.where(low, sq, 0.0), axis=1, keepdims=True)
        high_sum = jnp.sum(jnp.where(low, 0.0, sq), axis=1, keepdims=True)
        inverse = jnp.where(
            low,
            lax.rsqrt(low_sum * (1.0 / HEAD_SIZE) + eps_norm),
            lax.rsqrt(high_sum * (1.0 / HEAD_SIZE) + eps_norm),
        )
        turned = turn(vals * inverse * q_gain, q_base * (rows // GRID_ROW_WIDTH) + r)
        top, rest = split(turned * HEAD_SIZE ** (-0.5))
        qcat[at, :] = jnp.where(low, top, pltpu.roll(rest, HEAD_SIZE, 1)).astype(BF)
        later = span(q_tokens + r * GRID_ROW_WIDTH, GRID_ROW_WIDTH, GRID_ROW_WIDTH)
        qcat[later, :] = jnp.where(low, pltpu.roll(top, HEAD_SIZE, 1), rest).astype(BF)

    own_q.wait()

    def q_take(d):
        s = rem(head_at + kv_heads - d, kv_heads)
        dst = qbuf.at[span(s * rows, rows, rows)]

        @pl.when(d > 0)
        def _():
            remote(dst, dst, q_ss.at[d], q_rs.at[d], (q_base + s, core)).wait_recv()

        for r in range(rows // GRID_ROW_WIDTH):
            make_q(s * (rows // GRID_ROW_WIDTH) + r)

    loop(0, kv_heads, q_take)
    twin_first(up_part, *gate_next).start()
    loop(plane, later, lambda d: w_copy(d, up_part, *gate_sems).start())
    steps = rows // GRID_ROW_WIDTH

    def make_k(r):
        at = span(r * GRID_ROW_WIDTH, GRID_ROW_WIDTH, GRID_ROW_WIDTH)
        vals = kvbuf[at, :].astype(F32)
        total = jnp.sum(jnp.where(low, vals * vals, 0.0), axis=1, keepdims=True)
        turned = turn(
            vals * lax.rsqrt(total * (1.0 / HEAD_SIZE) + eps_norm) * k_gain, r
        )
        top, rest = split(turned)
        kcat[at, :LANES] = jnp.where(low, top, pltpu.roll(top, HEAD_SIZE, 1)).astype(BF)
        kcat[at, LANES:] = jnp.where(low, rest, pltpu.roll(rest, HEAD_SIZE, 1)).astype(BF)

    own_kv.wait()

    def kv_take(d):
        s = rem(sp + n - d, n)
        dst = kvbuf.at[span(s * rows, rows, rows)]

        @pl.when(d > 0)
        def _():
            remote(dst, dst, kv_ss.at[d], kv_rs.at[d], (s, core)).wait_recv()

        for r in range(steps):
            make_k(s * steps + r)

    loop(0, n, kv_take)
    loop(1, plane, lambda d: pass_on(d, up_part, *gate_sems, *gate_next))

    def o_copy(d):
        k = rem(head_at + d, kv_heads)
        return remote(
            att_s.at[span(k * rows, rows, rows)], attbuf.at[:, lane_block(head_at)],
            o_ss.at[d], o_rs.at[d], (q_base + k, core),
        )

    low_rows = lax.broadcasted_iota(jnp.int32, (rows, LANES), 1) < HEAD_SIZE

    def attend(k):
        both = jnp.concatenate(
            [qcat[span(k * rows, rows, rows), :], qcat[span(q_tokens + k * rows, rows, rows), :]],
            axis=0,
        )
        scores = nt(jnp.concatenate([both, both], axis=1), kcat[...])
        shifted = jnp.exp(scores - jnp.max(scores, axis=1, keepdims=True))
        total = jnp.sum(shifted, axis=1, keepdims=True)
        summed = jnp.dot(shifted.astype(BF), kvbuf[...], preferred_element_type=F32) / total
        return jnp.where(
            low_rows, pltpu.roll(summed[:rows], HEAD_SIZE, 1), summed[rows:]
        ).astype(BF)

    def attend_send(d):
        k = rem(head_at + d, kv_heads)
        att_s[span(k * rows, rows, rows), :] = attend(k)

        @pl.when(d < kv_heads)
        def _():
            o_copy(d).start()

    loop(1, kv_heads + 1, attend_send)
    attbuf[:, lane_block(head_at)] = att_s[span(head_at * rows, rows, rows), :]

    def o_wait(d):
        s = rem(head_at + kv_heads - d, kv_heads)
        dst = attbuf.at[:, lane_block(s)]
        remote(dst, dst, o_ss.at[d], o_rs.at[d], (q_base + s, core)).wait_recv()

    loop(1, kv_heads, o_wait)

    wo_copy.wait()
    po_s[...] = jnp.dot(attbuf[...], wo_buf[...], preferred_element_type=F32).astype(BF)
    po_copy = remote(
        po_s.at[span(mate * half_rows, half_rows, half_rows)], po_r, po_sem.at[0], po_sem.at[1],
        (sp, mate),
    )
    po_copy.start()
    mine = span(core * half_rows, half_rows, half_rows)
    base = x_ref[mine, :].astype(F32) + po_s[mine, :].astype(F32)
    po_copy.wait_recv()
    middle = base + po_r[...].astype(F32)
    mid[...] = middle
    scaled = lax.rsqrt(jnp.mean(middle * middle, axis=1, keepdims=True) + eps_norm)
    normed = (middle * scaled * fg_ref[...]).astype(BF)

    def slot(k, c):
        return allnorm.at[span(k * rows + c * half_rows, half_rows, half_rows)]

    allnorm[span(member * rows + core * half_rows, half_rows, half_rows), :] = normed

    def ag_copy(d):
        to = ahead(rem(d, plane)) if d != plane else ahead(d)
        of = member if d <= plane else (1 - wing) * plane + place
        return remote(
            slot(of, core), slot(of, core), ag_ss.at[d], ag_rs.at[d], (chip(to, side), core)
        )

    def fw_copy(d):
        s = behind(d)
        return remote(slot(s, core), slot(s, core), fw_ss.at[d], fw_rs.at[d], (sp, mate))

    def ag_wait(d):
        s = behind(d)
        remote(slot(s, core), slot(s, core), ag_ss.at[d], ag_rs.at[d], (sp, mate)).wait_recv()
        fw_copy(d).start()

    ag_copy(plane).start()
    for d in range(1, plane):
        ag_copy(d).start()
    fw_copy(0).start()

    own_w.wait()
    loop(later, group, lambda d: w_copy(d, up_part, *gate_sems).start())
    twin_first(down_part, *down_next).start()
    loop(1, plane, lambda d: pass_on(d, down_part, *down_sems, *down_next))
    loop(plane, later, lambda d: pass_on(d, up_part, *gate_sems, *gate_next))
    ag_wait(plane)
    for d in range(plane + 1, group):
        ag_copy(d).start()
    loop(plane, group, lambda d: w_copy(d, down_part, *down_sems).start())
    loop(later, group, lambda d: pass_on(d, up_part, *gate_sems, *gate_next))

    def up(block):
        both = nt(block, wrecv[: 2 * units, :]).astype(BF).astype(F32)
        return both[:, :units], both[:, units:]

    seg = plane * rows
    pitch = seg + 16

    def row_of(m):
        return (m // plane) * pitch + rem(m, plane) * rows

    def take(d):
        @pl.when(jnp.logical_and(d > 0, d != plane))
        def _():
            ag_wait(d)

    def mate_wait(d):
        s = behind(d)
        remote(slot(s, mate), slot(s, mate), fw_ss.at[d], fw_rs.at[d], (sp, mate)).wait_recv()

    def up_rows(k):
        side_at = rem(wing + k, 2)
        loop(k * plane, (k + 1) * plane, mate_wait)
        gate, value = up(allnorm[span(side_at * seg, seg, rows), :])
        at = span(side_at * pitch + 8, seg, 8)
        pre_g[at, :] = gate
        pre_v[at, :] = value

    loop(0, group, take)
    loop(0, group, lambda d: twin_wait(d, up_part, *gate_next))
    loop(plane, group, lambda d: pass_on(d, down_part, *down_sems, *down_next))
    loop(0, 2, up_rows)

    edge_at = (8, 8 + seg - 1, pitch + 8, pitch + 8 + seg - 1)
    edge_s[...] = jnp.concatenate(
        [
            jnp.concatenate([pre[k : k + 1, :] for k in edge_at] * 2, axis=0)
            for pre in (pre_g, pre_v)
        ],
        axis=0,
    )
    edge_copy = remote(edge_s, edge_r, h_sem.at[0], h_sem.at[1], (twin, core))
    edge_copy.start()
    loop(0, group, lambda d: twin_wait(d, down_part, *down_next))
    edge_copy.wait_recv()
    for pre, first_row in ((pre_g, 0), (pre_v, 8)):
        near = [
            jnp.broadcast_to(edge_r[first_row + k : first_row + k + 1, :], (8, units))
            for k in range(4)
        ]
        none = jnp.zeros((8, units), F32)
        pre[0:8, :] = jnp.where(side == 0, none, near[1])
        pre[8 + seg : pitch, :] = jnp.where(side == 0, near[0], near[2])
        pre[pitch : pitch + 8, :] = jnp.where(side == 0, near[1], near[3])
        pre[pitch + 8 + seg :, :] = jnp.where(side == 0, near[2], none)

    def convolve(ref, taps, k):
        block = ref[span(row_of(k), rows + 16, 8), :]
        return (
            taps[0:1, :] * block[7 : 7 + rows]
            + taps[1:2, :] * block[8 : 8 + rows]
            + taps[2:3, :] * block[9 : 9 + rows]
        )

    def dd_copy(d):
        return remote(
            part.at[d, span(mate * half_rows, half_rows, half_rows)], ddbuf.at[d],
            dd_ss.at[d], dd_rs.at[d], (sp, mate),
        )

    def c_copy(d, to):
        return remote(rs_s.at[d], rs_r.at[d], c_ss.at[d], c_rs.at[d], (chip(to, side), core))

    def c_near(d):
        return c_copy(d, ahead(rem(d, plane)))

    quarter_rows = half_rows // 2

    def c_half(d, h, to):
        at = span(h * quarter_rows, quarter_rows, quarter_rows)
        return remote(
            rs_s.at[d, at], rs_r.at[d, at], ch_ss.at[2 * d + h], ch_rs.at[2 * d + h],
            (chip(to, side), core),
        )

    def c_cross(d, h):
        return c_half(d, h, ahead(rem(d, plane)))

    def combine(d):
        dd_copy(d).wait_recv()
        return part[d, mine, :].astype(F32) + ddbuf[d].astype(F32)

    def send_sum(d):
        rs_s[d] = combine(d).astype(BF)

        @pl.when(d < plane)
        def _():
            c_near(d).start()

        @pl.when(d > plane)
        def _():
            c_cross(d, 0).start()

    def order(j):
        return plane * (1 - j // plane) + rem(j + 1, plane)

    def down(j):
        d = order(j)
        k = ahead(d)
        gate = convolve(pre_g, cg_ref, k)
        value = convolve(pre_v, cv_ref, k)
        hidden = (gate / (1.0 + jnp.exp(-gate)) * value).astype(BF)
        part[d] = jnp.dot(hidden, wrecv[2 * units :, :], preferred_element_type=F32).astype(BF)
        dd_copy(d).start()
        last = order(jnp.maximum(j - 1, 0))

        @pl.when(jnp.logical_and(j > 0, rem(last, plane) > 0))
        def _():
            send_sum(last)

        @pl.when(j == plane)
        def _():
            loop(plane + 1, group, lambda k: c_cross(k, 1).start())

    loop(0, group, down)

    def add_in(d):
        remote(rs_r.at[d], rs_r.at[d], c_ss.at[d], c_rs.at[d], (sp, mate)).wait_recv()
        own_sum[...] = own_sum[...] + rs_r[d].astype(F32)

    own_sum[...] = combine(plane)
    far = (1 - wing) * plane + place

    def far_send(h):
        at = span(h * quarter_rows, quarter_rows, quarter_rows)

        def half_in(d):
            c_cross(d, h).wait_recv()
            own_sum[at, :] = own_sum[at, :] + rs_r[d, at, :].astype(F32)

        loop(plane + 1, group, half_in)
        rs_s[plane, at, :] = own_sum[at, :].astype(BF)
        c_half(plane, h, far).start()

    loop(0, 2, far_send)
    own_sum[...] = mid[...] + combine(0)
    loop(1, plane, add_in)

    def far_take(h):
        at = span(h * quarter_rows, quarter_rows, quarter_rows)
        c_half(plane, h, far).wait_recv()
        own_sum[at, :] = own_sum[at, :] + rs_r[plane, at, :].astype(F32)

    loop(0, 2, far_take)
    fin_s[...] = own_sum[...].astype(BF)
    fin_copy = remote(fin_s, fin_r, fin_sem.at[0], fin_sem.at[1], (sp, mate))
    fin_copy.start()
    out_ref[mine, :] = fin_s[...]

    loop(1, kv_heads, lambda d: q_copy(d).wait_send())
    loop(1, n, lambda d: kv_copy(d).wait_send())
    loop(1, group, lambda d: w_copy(d, up_part, *gate_sems).wait_send())
    loop(1, group, lambda d: w_copy(d, down_part, *down_sems).wait_send())
    loop(0, group, lambda d: twin_copy(d, up_part, *gate_next).wait_send())
    loop(0, group, lambda d: twin_copy(d, down_part, *down_next).wait_send())
    loop(1, kv_heads, lambda d: o_copy(d).wait_send())
    po_copy.wait_send()
    for d in range(1, group):
        ag_copy(d).wait_send()
    loop(0, group, lambda d: fw_copy(d).wait_send())
    edge_copy.wait_send()
    loop(0, group, lambda d: dd_copy(d).wait_send())
    loop(1, plane, lambda d: c_near(d).wait_send())
    for h in range(2):
        for d in range(plane + 1, group):
            c_cross(d, h).wait_send()
        c_half(plane, h, far).wait_send()
    fin_copy.wait_send()
    fin_copy.wait_recv()
    out_ref[span(mate * half_rows, half_rows, half_rows), :] = fin_r[...]


def rotary_tables(count):
    lanes = jnp.arange(LANES)
    length = HEAD_SIZE // 2
    rate_at = (lanes % (length // 2)).astype(F32)
    rates = 1.0 / theta ** (rate_at * 2.0 / length)
    angles = jnp.arange(count, dtype=F32)[:, None] * rates[None, :]
    sign = jnp.where(lanes % length < length // 2, -1.0, 1.0)
    return jnp.cos(angles), jnp.sin(angles) * sign[None, :]


def kernel_shards(
    n, x_rows, queries, keys, values, query_norm_gain, key_norm_gain, out_weight, ffn_gain,
    gate_weight, value_weight, conv_gate, conv_value, down_weight,
):
    rows, width = x_rows.shape
    kv_heads = keys.shape[1] // HEAD_SIZE
    plane = n // 4
    group = 2 * plane
    unit_local = gate_weight.shape[1]
    units = unit_local // group
    depth = gate_weight.shape[0]
    kv = jnp.concatenate(
        [keys.reshape(rows, kv_heads, HEAD_SIZE), values.reshape(rows, kv_heads, HEAD_SIZE)], axis=-1
    ).reshape(rows, kv_heads * LANES)
    turned = [
        w.T.reshape(group, units, depth) for w in (gate_weight, value_weight, down_weight)
    ]
    weights = jnp.concatenate(turned, axis=1)
    at = lax.axis_index("sp")
    chip = (at // group) * plane + rem(at, plane)
    taps = [lax.dynamic_slice_in_dim(t, chip * units, units, 1) for t in (conv_gate, conv_value)]
    cos, sin = rotary_tables(max(GRID_ROW_WIDTH, n * rows // GRID_ROW_WIDTH))
    tokens, q_tokens, span_rows = n * rows, kv_heads * rows, group * rows
    half_rows = rows // 2
    dma = pltpu.SemaphoreType.DMA
    vm = pltpu.VMEM
    scratch = [
        vm(out_weight.shape, BF), vm((tokens, LANES), BF), vm((q_tokens, LANES), BF), vm((tokens, 2 * LANES), BF),
        vm((2 * q_tokens, LANES), BF), vm((q_tokens, LANES), BF), vm((rows, kv_heads * LANES), BF),
        vm((rows, width), BF), vm((half_rows, width), BF), vm((half_rows, width), F32),
        vm((span_rows, width), BF), vm((16, units), F32),
        vm((16, units), F32), vm((3 * units, width), BF),
        vm((span_rows + 32, units), F32), vm((span_rows + 32, units), F32),
        vm((group, rows, width), BF), vm((group, half_rows, width), BF),
        vm((half_rows, width), F32), vm((group, half_rows, width), BF),
        vm((group, half_rows, width), BF), vm((half_rows, width), BF), vm((half_rows, width), BF),
        dma((4,)), dma((n,)), dma((n,)), dma((kv_heads,)), dma((kv_heads,)), *[dma((group,))] * 8,
        dma((kv_heads,)), dma((kv_heads,)), dma((2,)), dma((group,)), dma((group,)),
        dma((group,)), dma((group,)), dma((2 * group,)), dma((2 * group,)), dma((2,)),
        dma((group,)), dma((group,)),
        dma((group,)), dma((group,)), dma((2,)),
    ]
    args = (
        x_rows, queries, kv, query_norm_gain[None, :], key_norm_gain[None, :],
        cos, sin, out_weight, ffn_gain[None, :], weights, taps[0], taps[1],
    )
    return pl.pallas_call(
        lambda *refs: layer_kernel(n, *refs),
        out_shape=jax.ShapeDtypeStruct((rows, width), BF),
        in_specs=[
            pl.BlockSpec(memory_space=pl.ANY if a is out_weight else pltpu.VMEM) for a in args
        ],
        out_specs=pl.BlockSpec(memory_space=pltpu.VMEM),
        scratch_shapes=scratch,
        compiler_params=pltpu.CompilerParams(
            collective_id=0, has_side_effects=True, vmem_limit_bytes=60 * 2**20
        ),
        name="layer",
    )(*args)


def suits(mesh, sizes):
    n, pair = mesh.shape["sp"], mesh.shape["tp"]
    x_rows, queries, keys, gate = sizes
    if pair != 2 or n % 4:
        return False
    rows, group = x_rows[0] // n, n // 2
    heads = keys[1] // pair // HEAD_SIZE
    units = gate[1] // pair
    return (
        rows % GRID_ROW_WIDTH == 0
        and rows % 32 == 0
        and queries[1] == 2 * keys[1]
        and n % heads == 0
        and 2 * HEAD_SIZE == LANES
        and x_rows[1] == n * LANES
        and units % (16 * group) == 0
    )


def solution(mesh):
    placed = (
        P("sp", None),
        P("sp", "tp"),
        P("sp", "tp"),
        P("sp", "tp"),
        P(),
        P(),
        P("tp", None),
        P(),
        P("sp", "tp"),
        P("sp", "tp"),
        P(None, "tp"),
        P(None, "tp"),
        P("sp", "tp"),
    )
    def run(*arrays):
        n = mesh.shape["sp"]
        fits = suits(mesh, [arrays[k].shape for k in (0, 1, 2, 8)])
        local = functools.partial(kernel_shards, n) if fits else shards
        return jax.shard_map(
            local, mesh=mesh, in_specs=placed, out_specs=P("sp", None), check_vma=False
        )(*arrays)

    return run
```

```python
import functools
import math

import jax
import jax.numpy as jnp
from jax import lax
from jax.experimental import pallas as pl
from jax.experimental.pallas import tpu as pltpu
from jax.sharding import PartitionSpec as P

HEAD_SIZE = 64
GRID_ROW_WIDTH = 64


eps_norm = 1e-06
theta = 10000.0


def with_halo(cells, sides, width):
    for axis, dim in sides:
        count = lax.axis_size(axis)
        ends = count - 1
        head = lax.slice_in_dim(cells, 0, width, axis=dim)
        tail = lax.slice_in_dim(cells, cells.shape[dim] - width, cells.shape[dim], axis=dim)
        cells = jnp.concatenate(
            [
                lax.ppermute(tail, axis, [(i, (i + 1) % count) for i in range(ends)]),
                cells,
                lax.ppermute(head, axis, [((i + 1) % count, i) for i in range(ends)]),
            ],
            axis=dim,
        )
    return cells


def per_head_norm(head_block, gain_vec):
    wide_vals = head_block.astype(jnp.float32)
    inverse_rms = lax.rsqrt(jnp.mean(wide_vals * wide_vals, axis=-1, keepdims=True) + eps_norm)
    return wide_vals * inverse_rms * gain_vec


def turn_half(half_vec, places):
    quarter_len = half_vec.shape[-1] // 2
    inverse_rates = 1.0 / theta ** (
        jnp.arange(quarter_len, dtype=jnp.float32) * 2.0 / half_vec.shape[-1]
    )
    angles = places.astype(jnp.float32)[:, None] * inverse_rates[None, :]
    angles = jnp.concatenate([angles, angles], axis=-1)[:, None, :]
    front_part = half_vec[..., :quarter_len]
    back_part = half_vec[..., quarter_len:]
    return half_vec * jnp.cos(angles) + jnp.concatenate(
        [-back_part, front_part], axis=-1
    ) * jnp.sin(angles)


def apply_rotary(normed_heads, token_positions):
    half_point = normed_heads.shape[-1] // 2
    grid_row = token_positions // GRID_ROW_WIDTH
    grid_col = token_positions % GRID_ROW_WIDTH
    return jnp.concatenate(
        [
            turn_half(normed_heads[..., :half_point], grid_row),
            turn_half(normed_heads[..., half_point:], grid_col),
        ],
        axis=-1,
    )


def row_norm(rows_wide, gain_vec):
    inverse_rms = lax.rsqrt(jnp.mean(rows_wide * rows_wide, axis=-1, keepdims=True) + eps_norm)
    return (rows_wide * inverse_rms * gain_vec).astype(jnp.bfloat16)


def contract_units(left_rows, right_rows):
    return lax.dot_general(
        left_rows, right_rows, (((1,), (1,)), ((), ())), preferred_element_type=jnp.float32
    )


def shards(
    x_rows,
    queries,
    keys,
    values,
    query_norm_gain,
    key_norm_gain,
    out_weight,
    ffn_gain,
    gate_weight,
    value_weight,
    conv_gate,
    conv_value,
    down_weight,
):
    collected = (
        lax.all_gather(gate_weight, "sp", axis=0, tiled=True),
        lax.all_gather(value_weight, "sp", axis=0, tiled=True),
        lax.all_gather(down_weight, "sp", axis=0, tiled=True),
    )
    tokens_here = queries.shape[0]
    query_heads = queries.shape[1] // HEAD_SIZE
    key_heads = keys.shape[1] // HEAD_SIZE
    group_width = query_heads // key_heads
    lane_rows = group_width * tokens_here
    token_positions = lax.axis_index("sp") * tokens_here + jnp.arange(tokens_here, dtype=jnp.int32)
    rotated_queries = apply_rotary(
        per_head_norm(queries.reshape(tokens_here, query_heads, HEAD_SIZE), query_norm_gain),
        token_positions,
    )
    query_lanes = rotated_queries.reshape(tokens_here, key_heads, group_width, HEAD_SIZE).transpose(
        1, 2, 0, 3
    )
    query_lanes = query_lanes.reshape(key_heads, lane_rows, HEAD_SIZE) * HEAD_SIZE ** (-0.5)
    start_state = (
        jnp.full((key_heads, lane_rows), -1e30, jnp.float32),
        jnp.zeros((key_heads, lane_rows), jnp.float32),
        jnp.zeros((key_heads, lane_rows, HEAD_SIZE), jnp.float32),
    )
    key_piece = lax.all_gather(keys, "sp", axis=0, tiled=True)
    value_piece = lax.all_gather(values, "sp", axis=0, tiled=True)
    row_count = key_piece.shape[0]
    key_places = jnp.arange(row_count, dtype=jnp.int32)
    turned = apply_rotary(
        per_head_norm(key_piece.reshape(row_count, key_heads, HEAD_SIZE), key_norm_gain), key_places
    )
    key_span = math.gcd(row_count, 2048)
    span_count = row_count // key_span
    turned = turned.reshape(span_count, key_span, key_heads, HEAD_SIZE)
    value_matrix = value_piece.reshape(span_count, key_span, key_heads, HEAD_SIZE)

    def one_span(state_now, inputs):
        running_top, denominator, weighted = state_now
        key_block, value_block = inputs
        scores = jnp.einsum("hrd,shd->hrs", query_lanes, key_block, precision=lax.Precision.HIGHEST)
        new_top = jnp.maximum(running_top, jnp.max(scores, axis=-1))
        factor = jnp.exp(running_top - new_top)
        weights = jnp.exp(scores - new_top[..., None])
        denominator = denominator * factor + jnp.sum(weights, axis=-1)
        weighted = weighted * factor[..., None] + jnp.einsum(
            "hrs,shd->hrd",
            weights.astype(jnp.bfloat16),
            value_block,
            preferred_element_type=jnp.float32,
        )
        return ((new_top, denominator, weighted), None)

    folded_state, _ = lax.scan(one_span, start_state, (turned, value_matrix))
    running_top, denominator, weighted = folded_state
    attended = (weighted / denominator[..., None]).reshape(
        key_heads, group_width, tokens_here, HEAD_SIZE
    )
    attended = (
        attended.transpose(2, 0, 1, 3)
        .reshape(tokens_here, query_heads * HEAD_SIZE)
        .astype(jnp.bfloat16)
    )
    share_rows = tokens_here // lax.axis_size("tp")
    head_share = lax.psum_scatter(
        jnp.dot(attended, out_weight, preferred_element_type=jnp.float32).astype(jnp.bfloat16),
        "tp",
        scatter_dimension=0,
        tiled=True,
    ).astype(jnp.float32)
    own_rows = lax.dynamic_slice_in_dim(x_rows, lax.axis_index("tp") * share_rows, share_rows, 0)
    middle_rows = own_rows.astype(jnp.float32) + head_share
    normed = lax.all_gather(row_norm(middle_rows, ffn_gain), "tp", axis=0, tiled=True)
    unit_local = gate_weight.shape[1]
    gate_pre = jnp.dot(normed, collected[0], preferred_element_type=jnp.float32).astype(
        jnp.bfloat16
    )
    value_pre = jnp.dot(normed, collected[1], preferred_element_type=jnp.float32).astype(
        jnp.bfloat16
    )
    joined = jnp.concatenate([gate_pre, value_pre], axis=1)
    padded = with_halo(joined, (("sp", 0),), 1).astype(jnp.float32)
    conv_taps = jnp.concatenate([conv_gate, conv_value], axis=1)
    convolved = conv_taps[0] * padded[:-2] + conv_taps[1] * padded[1:-1] + conv_taps[2] * padded[2:]
    hidden = (jax.nn.silu(convolved[:, :unit_local]) * convolved[:, unit_local:]).astype(
        jnp.bfloat16
    )
    unit_share = lax.psum_scatter(
        contract_units(hidden, collected[2]).astype(jnp.bfloat16),
        "tp",
        scatter_dimension=0,
        tiled=True,
    ).astype(jnp.float32)
    finished = (middle_rows + unit_share).astype(jnp.bfloat16)
    return lax.all_gather(finished, "tp", axis=0, tiled=True)

LANES = 128
MESH = pl.DeviceIdType.MESH
BF = jnp.bfloat16
F32 = jnp.float32


def rem(a, b):
    return a % b if isinstance(a, int) else lax.rem(a, b)


def nt(left, right):
    return lax.dot_general(left, right, (((1,), (1,)), ((), ())), preferred_element_type=F32)


def layer_kernel(
    n, x_ref, q_ref, kv_ref, qg_ref, kg_ref, cos_ref, sin_ref, wo_ref, fg_ref, wg_ref, wv_ref, wd_ref,
    cg_ref, cv_ref, out_ref,
    wo_buf, kvbuf, qbuf, kcat, qcat, att_s, attbuf, po_s, po_r, mid, allnorm, edge_s, edge_r, wrecv,
    pre_g, pre_v, part, ddbuf, own_sum, rs_s, rs_r, fin_s, fin_r,
    loc, kv_ss, kv_rs, q_ss, q_rs, w_ss, w_rs, wv_ss, wv_rs, wf_ss, wf_rs, dw_ss, dw_rs, df_ss, df_rs, o_ss, o_rs, po_sem, ag_ss, ag_rs, fw_ss, fw_rs,
    ch_ss, ch_rs, h_sem, dd_ss, dd_rs, c_ss, c_rs, fin_sem,
):
    sp = lax.axis_index("sp")
    core = lax.axis_index("tp")
    mate = 1 - core
    rows = x_ref.shape[0]
    half_rows = rows // 2
    width = x_ref.shape[1]
    kv_heads = kv_ref.shape[1] // LANES
    plane = n // 4
    group = 2 * plane
    tokens = n * rows
    q_tokens = kv_heads * rows
    units = wd_ref.shape[1]
    head_at = rem(sp, kv_heads)
    q_base = sp - head_at
    place = rem(sp, plane)
    side = rem(sp // plane, 2)
    wing = sp // (2 * plane)
    member = wing * plane + place

    def chip(m, at_side):
        return (m // plane) * (2 * plane) + at_side * plane + rem(m, plane)

    def ahead(d):
        return rem(wing + d // plane, 2) * plane + rem(place + rem(d, plane), plane)

    def behind(d):
        return rem(wing + d // plane, 2) * plane + rem(
            place + plane - rem(d, plane), plane
        )

    twin = chip(member, 1 - side)

    def remote(src, dst, ss, rs, device):
        return pltpu.make_async_remote_copy(
            src_ref=src, dst_ref=dst, send_sem=ss, recv_sem=rs, device_id=device, device_id_type=MESH
        )

    def lane_block(k):
        return pl.ds(pl.multiple_of(k * LANES, LANES), LANES)

    def span(start, size, unit):
        return pl.ds(pl.multiple_of(start, unit), size)

    def loop(lo, hi, fn):
        def step(k, carry):
            fn(k)
            return carry

        lax.fori_loop(lo, hi, step, 0)

    barrier = pltpu.get_barrier_semaphore()

    def greet(d):
        t = rem(sp + d, n)
        pl.semaphore_signal(barrier, inc=1, device_id=(t, core), device_id_type=MESH)

    loop(1, n, greet)
    pl.semaphore_signal(barrier, inc=1, device_id=(sp, mate), device_id_type=MESH)
    pl.semaphore_wait(barrier, n)

    def q_copy(d):
        t = q_base + rem(head_at + d, kv_heads)
        return remote(
            q_ref.at[:, lane_block(t - q_base)], qbuf.at[span(head_at * rows, rows, rows)],
            q_ss.at[d], q_rs.at[d], (t, core),
        )

    def kv_copy(d):
        t = rem(sp + d, n)
        return remote(
            kv_ref.at[:, lane_block(rem(t, kv_heads))], kvbuf.at[span(sp * rows, rows, rows)],
            kv_ss.at[d], kv_rs.at[d], (t, core),
        )

    up_part, down_part = slice(0, 2 * units), slice(2 * units, 3 * units)

    gate_part, value_part = slice(0, units), slice(units, 2 * units)

    def w_copy(d, src, part_at, ss, rs):
        m = ahead(d)
        return remote(
            src.at[m], wrecv.at[part_at, lane_block(sp)], ss.at[d], rs.at[d], (chip(m, side), core)
        )

    def w_copies(d):
        return (
            w_copy(d, wg_ref, gate_part, w_ss, w_rs),
            w_copy(d, wv_ref, value_part, wv_ss, wv_rs),
            w_copy(d, wd_ref, down_part, dw_ss, dw_rs),
        )

    def up_send(d):
        for one in w_copies(d)[:2]:
            one.start()

    def down_send(d):
        w_copies(d)[2].start()

    own_parts = ((wg_ref, gate_part), (wv_ref, value_part), (wd_ref, down_part))

    def own_copy(k):
        src, part_at = own_parts[k]
        return pltpu.make_async_copy(
            src.at[member], wrecv.at[part_at, lane_block(sp)], loc.at[(2, 4, 5)[k]]
        )

    def twin_copy(d, part_at, ss, rs):
        at = wrecv.at[part_at, lane_block(chip(behind(d), side))]
        return remote(at, at, ss.at[d], rs.at[d], (twin, core))

    def land(d, part_at, rs):
        dst = wrecv.at[part_at, lane_block(chip(behind(d), side))]
        remote(dst, dst, w_ss.at[d], rs.at[d], (twin, core)).wait_recv()

    def up_pass(d):
        land(d, gate_part, w_rs)
        land(d, value_part, wv_rs)
        twin_copy(d, up_part, *gate_next).start()

    def down_pass(d):
        land(d, down_part, dw_rs)
        twin_copy(d, down_part, *down_next).start()

    def twin_wait(d, part_at, ss, rs):
        dst = wrecv.at[part_at, lane_block(chip(behind(d), 1 - side))]
        remote(dst, dst, ss.at[d], rs.at[d], (twin, core)).wait_recv()

    later = plane + plane // 2
    gate_next, down_next = (wf_ss, wf_rs), (df_ss, df_rs)

    own_q = pltpu.make_async_copy(
        q_ref.at[:, lane_block(head_at)], qbuf.at[span(head_at * rows, rows, rows)], loc.at[0]
    )
    own_kv = pltpu.make_async_copy(
        kv_ref.at[:, lane_block(head_at)], kvbuf.at[span(sp * rows, rows, rows)], loc.at[1]
    )
    own_q.start()
    wo_copy = pltpu.make_async_copy(wo_ref, wo_buf, loc.at[3])
    wo_copy.start()
    own_kv.start()
    loop(1, kv_heads, lambda d: q_copy(d).start())
    loop(1, n, lambda d: kv_copy(d).start())
    loop(1, plane, up_send)
    loop(1, plane, down_send)
    for k in range(3):
        own_copy(k).start()

    lane = lax.broadcasted_iota(jnp.int32, (GRID_ROW_WIDTH, LANES), 1)
    low = lane < HEAD_SIZE
    first = rem(lane, 2 * HEAD_SIZE // 4) < HEAD_SIZE // 4
    by_row = rem(lane, HEAD_SIZE) < HEAD_SIZE // 2

    def turn(vals, grid_row):
        cos = jnp.where(by_row, cos_ref[pl.ds(grid_row, 1), :], cos_ref[:GRID_ROW_WIDTH, :])
        sin = jnp.where(by_row, sin_ref[pl.ds(grid_row, 1), :], sin_ref[:GRID_ROW_WIDTH, :])
        quarter = HEAD_SIZE // 4
        swapped = jnp.where(
            first, pltpu.roll(vals, LANES - quarter, 1), pltpu.roll(vals, quarter, 1)
        )
        return vals * cos + swapped * sin

    q_gain = jnp.concatenate([qg_ref[...]] * 2, axis=1)
    k_gain = jnp.concatenate([kg_ref[...]] * 2, axis=1)

    def split(vals):
        top = vals.astype(BF).astype(F32)
        return top, (vals - top).astype(BF).astype(F32)

    def make_q(r):
        at = span(r * GRID_ROW_WIDTH, GRID_ROW_WIDTH, GRID_ROW_WIDTH)
        vals = qbuf[at, :].astype(F32)
        sq = vals * vals
        low_sum = jnp.sum(jnp.where(low, sq, 0.0), axis=1, keepdims=True)
        high_sum = jnp.sum(jnp.where(low, 0.0, sq), axis=1, keepdims=True)
        inverse = jnp.where(
            low,
            lax.rsqrt(low_sum * (1.0 / HEAD_SIZE) + eps_norm),
            lax.rsqrt(high_sum * (1.0 / HEAD_SIZE) + eps_norm),
        )
        turned = turn(vals * inverse * q_gain, q_base * (rows // GRID_ROW_WIDTH) + r)
        top, rest = split(turned * HEAD_SIZE ** (-0.5))
        qcat[at, :] = jnp.where(low, top, pltpu.roll(rest, HEAD_SIZE, 1)).astype(BF)
        later = span(q_tokens + r * GRID_ROW_WIDTH, GRID_ROW_WIDTH, GRID_ROW_WIDTH)
        qcat[later, :] = jnp.where(low, pltpu.roll(top, HEAD_SIZE, 1), rest).astype(BF)

    own_q.wait()

    def q_take(d):
        s = rem(head_at + kv_heads - d, kv_heads)
        dst = qbuf.at[span(s * rows, rows, rows)]

        @pl.when(d > 0)
        def _():
            remote(dst, dst, q_ss.at[d], q_rs.at[d], (q_base + s, core)).wait_recv()

        for r in range(rows // GRID_ROW_WIDTH):
            make_q(s * (rows // GRID_ROW_WIDTH) + r)

    loop(0, kv_heads, q_take)
    for k in range(3):
        own_copy(k).wait()
    twin_copy(0, up_part, *gate_next).start()
    loop(plane, later, up_send)
    steps = rows // GRID_ROW_WIDTH

    def make_k(r):
        at = span(r * GRID_ROW_WIDTH, GRID_ROW_WIDTH, GRID_ROW_WIDTH)
        vals = kvbuf[at, :].astype(F32)
        total = jnp.sum(jnp.where(low, vals * vals, 0.0), axis=1, keepdims=True)
        turned = turn(
            vals * lax.rsqrt(total * (1.0 / HEAD_SIZE) + eps_norm) * k_gain, r
        )
        top, rest = split(turned)
        kcat[at, :LANES] = jnp.where(low, top, pltpu.roll(top, HEAD_SIZE, 1)).astype(BF)
        kcat[at, LANES:] = jnp.where(low, rest, pltpu.roll(rest, HEAD_SIZE, 1)).astype(BF)

    own_kv.wait()

    def kv_take(d):
        s = rem(sp + n - d, n)
        dst = kvbuf.at[span(s * rows, rows, rows)]

        @pl.when(d > 0)
        def _():
            remote(dst, dst, kv_ss.at[d], kv_rs.at[d], (s, core)).wait_recv()

        for r in range(steps):
            make_k(s * steps + r)

    loop(0, n, kv_take)
    loop(1, plane, up_pass)

    def o_copy(d):
        k = rem(head_at + d, kv_heads)
        return remote(
            att_s.at[span(k * rows, rows, rows)], attbuf.at[:, lane_block(head_at)],
            o_ss.at[d], o_rs.at[d], (q_base + k, core),
        )

    low_rows = lax.broadcasted_iota(jnp.int32, (rows, LANES), 1) < HEAD_SIZE

    def attend(k):
        both = jnp.concatenate(
            [qcat[span(k * rows, rows, rows), :], qcat[span(q_tokens + k * rows, rows, rows), :]],
            axis=0,
        )
        scores = nt(jnp.concatenate([both, both], axis=1), kcat[...])
        shifted = jnp.exp(scores - jnp.max(scores, axis=1, keepdims=True))
        total = jnp.sum(shifted, axis=1, keepdims=True)
        summed = jnp.dot(shifted.astype(BF), kvbuf[...], preferred_element_type=F32) / total
        return jnp.where(
            low_rows, pltpu.roll(summed[:rows], HEAD_SIZE, 1), summed[rows:]
        ).astype(BF)

    def attend_send(d):
        k = rem(head_at + d, kv_heads)
        att_s[span(k * rows, rows, rows), :] = attend(k)

        @pl.when(d < kv_heads)
        def _():
            o_copy(d).start()

    loop(1, kv_heads + 1, attend_send)
    attbuf[:, lane_block(head_at)] = att_s[span(head_at * rows, rows, rows), :]

    def o_wait(d):
        s = rem(head_at + kv_heads - d, kv_heads)
        dst = attbuf.at[:, lane_block(s)]
        remote(dst, dst, o_ss.at[d], o_rs.at[d], (q_base + s, core)).wait_recv()

    loop(1, kv_heads, o_wait)

    wo_copy.wait()
    po_s[...] = jnp.dot(attbuf[...], wo_buf[...], preferred_element_type=F32).astype(BF)
    po_copy = remote(
        po_s.at[span(mate * half_rows, half_rows, half_rows)], po_r, po_sem.at[0], po_sem.at[1],
        (sp, mate),
    )
    po_copy.start()
    mine = span(core * half_rows, half_rows, half_rows)
    base = x_ref[mine, :].astype(F32) + po_s[mine, :].astype(F32)
    po_copy.wait_recv()
    middle = base + po_r[...].astype(F32)
    mid[...] = middle
    scaled = lax.rsqrt(jnp.mean(middle * middle, axis=1, keepdims=True) + eps_norm)
    normed = (middle * scaled * fg_ref[...]).astype(BF)

    def slot(k, c):
        return allnorm.at[span(k * rows + c * half_rows, half_rows, half_rows)]

    allnorm[span(member * rows + core * half_rows, half_rows, half_rows), :] = normed

    def ag_copy(d):
        to = ahead(rem(d, plane)) if d != plane else ahead(d)
        of = member if d <= plane else (1 - wing) * plane + place
        return remote(
            slot(of, core), slot(of, core), ag_ss.at[d], ag_rs.at[d], (chip(to, side), core)
        )

    def fw_copy(d):
        s = behind(d)
        return remote(slot(s, core), slot(s, core), fw_ss.at[d], fw_rs.at[d], (sp, mate))

    def ag_wait(d):
        s = behind(d)
        remote(slot(s, core), slot(s, core), ag_ss.at[d], ag_rs.at[d], (sp, mate)).wait_recv()
        fw_copy(d).start()

    ag_copy(plane).start()
    for d in range(1, plane):
        ag_copy(d).start()
    fw_copy(0).start()

    loop(later, group, up_send)
    twin_copy(0, down_part, *down_next).start()
    loop(1, plane, down_pass)
    loop(plane, later, up_pass)
    ag_wait(plane)
    for d in range(plane + 1, group):
        ag_copy(d).start()
    loop(plane, group, down_send)
    loop(later, group, up_pass)

    def up(block):
        both = nt(block, wrecv[: 2 * units, :]).astype(BF).astype(F32)
        return both[:, :units], both[:, units:]

    seg = plane * rows
    pitch = seg + 16

    def row_of(m):
        return (m // plane) * pitch + rem(m, plane) * rows

    def take(d):
        @pl.when(jnp.logical_and(d > 0, d != plane))
        def _():
            ag_wait(d)

    def mate_wait(d):
        s = behind(d)
        remote(slot(s, mate), slot(s, mate), fw_ss.at[d], fw_rs.at[d], (sp, mate)).wait_recv()

    def up_rows(k):
        side_at = rem(wing + k, 2)
        loop(k * plane, (k + 1) * plane, mate_wait)
        gate, value = up(allnorm[span(side_at * seg, seg, rows), :])
        at = span(side_at * pitch + 8, seg, 8)
        pre_g[at, :] = gate
        pre_v[at, :] = value

    loop(0, group, take)
    loop(0, group, lambda d: twin_wait(d, up_part, *gate_next))
    loop(plane, group, down_pass)
    loop(0, 2, up_rows)

    edge_at = (8, 8 + seg - 1, pitch + 8, pitch + 8 + seg - 1)
    edge_s[...] = jnp.concatenate(
        [
            jnp.concatenate([pre[k : k + 1, :] for k in edge_at] * 2, axis=0)
            for pre in (pre_g, pre_v)
        ],
        axis=0,
    )
    edge_copy = remote(edge_s, edge_r, h_sem.at[0], h_sem.at[1], (twin, core))
    edge_copy.start()
    loop(0, group, lambda d: twin_wait(d, down_part, *down_next))
    edge_copy.wait_recv()
    for pre, first_row in ((pre_g, 0), (pre_v, 8)):
        near = [
            jnp.broadcast_to(edge_r[first_row + k : first_row + k + 1, :], (8, units))
            for k in range(4)
        ]
        none = jnp.zeros((8, units), F32)
        pre[0:8, :] = jnp.where(side == 0, none, near[1])
        pre[8 + seg : pitch, :] = jnp.where(side == 0, near[0], near[2])
        pre[pitch : pitch + 8, :] = jnp.where(side == 0, near[1], near[3])
        pre[pitch + 8 + seg :, :] = jnp.where(side == 0, near[2], none)

    def convolve(ref, taps, k):
        block = ref[span(row_of(k), rows + 16, 8), :]
        return (
            taps[0:1, :] * block[7 : 7 + rows]
            + taps[1:2, :] * block[8 : 8 + rows]
            + taps[2:3, :] * block[9 : 9 + rows]
        )

    def dd_copy(d):
        return remote(
            part.at[d, span(mate * half_rows, half_rows, half_rows)], ddbuf.at[d],
            dd_ss.at[d], dd_rs.at[d], (sp, mate),
        )

    def c_copy(d, to):
        return remote(rs_s.at[d], rs_r.at[d], c_ss.at[d], c_rs.at[d], (chip(to, side), core))

    def c_near(d):
        return c_copy(d, ahead(rem(d, plane)))

    quarter_rows = half_rows // 2

    def c_half(d, h, to):
        at = span(h * quarter_rows, quarter_rows, quarter_rows)
        return remote(
            rs_s.at[d, at], rs_r.at[d, at], ch_ss.at[2 * d + h], ch_rs.at[2 * d + h],
            (chip(to, side), core),
        )

    def c_cross(d, h):
        return c_half(d, h, ahead(rem(d, plane)))

    def combine(d):
        dd_copy(d).wait_recv()
        return part[d, mine, :].astype(F32) + ddbuf[d].astype(F32)

    def send_sum(d):
        rs_s[d] = combine(d).astype(BF)

        @pl.when(d < plane)
        def _():
            c_near(d).start()

        @pl.when(d > plane)
        def _():
            c_cross(d, 0).start()

    def order(j):
        return plane * (1 - j // plane) + rem(j + 1, plane)

    def down(j):
        d = order(j)
        k = ahead(d)
        gate = convolve(pre_g, cg_ref, k)
        value = convolve(pre_v, cv_ref, k)
        hidden = (gate / (1.0 + jnp.exp(-gate)) * value).astype(BF)
        part[d] = jnp.dot(hidden, wrecv[2 * units :, :], preferred_element_type=F32).astype(BF)
        dd_copy(d).start()
        last = order(jnp.maximum(j - 1, 0))

        @pl.when(jnp.logical_and(j > 0, rem(last, plane) > 0))
        def _():
            send_sum(last)

        @pl.when(j == plane)
        def _():
            loop(plane + 1, group, lambda k: c_cross(k, 1).start())

    loop(0, group, down)

    def add_in(d):
        remote(rs_r.at[d], rs_r.at[d], c_ss.at[d], c_rs.at[d], (sp, mate)).wait_recv()
        own_sum[...] = own_sum[...] + rs_r[d].astype(F32)

    own_sum[...] = combine(plane)
    far = (1 - wing) * plane + place

    def far_send(h):
        at = span(h * quarter_rows, quarter_rows, quarter_rows)

        def half_in(d):
            c_cross(d, h).wait_recv()
            own_sum[at, :] = own_sum[at, :] + rs_r[d, at, :].astype(F32)

        loop(plane + 1, group, half_in)
        rs_s[plane, at, :] = own_sum[at, :].astype(BF)
        c_half(plane, h, far).start()

    loop(0, 2, far_send)
    own_sum[...] = mid[...] + combine(0)
    loop(1, plane, add_in)

    def far_take(h):
        at = span(h * quarter_rows, quarter_rows, quarter_rows)
        c_half(plane, h, far).wait_recv()
        own_sum[at, :] = own_sum[at, :] + rs_r[plane, at, :].astype(F32)

    loop(0, 2, far_take)
    fin_s[...] = own_sum[...].astype(BF)
    fin_copy = remote(fin_s, fin_r, fin_sem.at[0], fin_sem.at[1], (sp, mate))
    fin_copy.start()
    out_ref[mine, :] = fin_s[...]

    loop(1, kv_heads, lambda d: q_copy(d).wait_send())
    loop(1, n, lambda d: kv_copy(d).wait_send())

    def w_sent(d):
        for one in w_copies(d):
            one.wait_send()

    loop(1, group, w_sent)
    loop(0, group, lambda d: twin_copy(d, up_part, *gate_next).wait_send())
    loop(0, group, lambda d: twin_copy(d, down_part, *down_next).wait_send())
    loop(1, kv_heads, lambda d: o_copy(d).wait_send())
    po_copy.wait_send()
    for d in range(1, group):
        ag_copy(d).wait_send()
    loop(0, group, lambda d: fw_copy(d).wait_send())
    edge_copy.wait_send()
    loop(0, group, lambda d: dd_copy(d).wait_send())
    loop(1, plane, lambda d: c_near(d).wait_send())
    for h in range(2):
        for d in range(plane + 1, group):
            c_cross(d, h).wait_send()
        c_half(plane, h, far).wait_send()
    fin_copy.wait_send()
    fin_copy.wait_recv()
    out_ref[span(mate * half_rows, half_rows, half_rows), :] = fin_r[...]


def rotary_tables(count):
    lanes = jnp.arange(LANES)
    length = HEAD_SIZE // 2
    rate_at = (lanes % (length // 2)).astype(F32)
    rates = 1.0 / theta ** (rate_at * 2.0 / length)
    angles = jnp.arange(count, dtype=F32)[:, None] * rates[None, :]
    sign = jnp.where(lanes % length < length // 2, -1.0, 1.0)
    return jnp.cos(angles), jnp.sin(angles) * sign[None, :]


def kernel_shards(
    n, x_rows, queries, keys, values, query_norm_gain, key_norm_gain, out_weight, ffn_gain,
    gate_weight, value_weight, conv_gate, conv_value, down_weight,
):
    rows, width = x_rows.shape
    kv_heads = keys.shape[1] // HEAD_SIZE
    plane = n // 4
    group = 2 * plane
    unit_local = gate_weight.shape[1]
    units = unit_local // group
    depth = gate_weight.shape[0]
    kv = jnp.concatenate(
        [keys.reshape(rows, kv_heads, HEAD_SIZE), values.reshape(rows, kv_heads, HEAD_SIZE)], axis=-1
    ).reshape(rows, kv_heads * LANES)
    turned = [
        w.T.reshape(group, units, depth) for w in (gate_weight, value_weight, down_weight)
    ]
    at = lax.axis_index("sp")
    chip = (at // group) * plane + rem(at, plane)
    taps = [lax.dynamic_slice_in_dim(t, chip * units, units, 1) for t in (conv_gate, conv_value)]
    cos, sin = rotary_tables(max(GRID_ROW_WIDTH, n * rows // GRID_ROW_WIDTH))
    tokens, q_tokens, span_rows = n * rows, kv_heads * rows, group * rows
    half_rows = rows // 2
    dma = pltpu.SemaphoreType.DMA
    vm = pltpu.VMEM
    scratch = [
        vm(out_weight.shape, BF), vm((tokens, LANES), BF), vm((q_tokens, LANES), BF), vm((tokens, 2 * LANES), BF),
        vm((2 * q_tokens, LANES), BF), vm((q_tokens, LANES), BF), vm((rows, kv_heads * LANES), BF),
        vm((rows, width), BF), vm((half_rows, width), BF), vm((half_rows, width), F32),
        vm((span_rows, width), BF), vm((16, units), F32),
        vm((16, units), F32), vm((3 * units, width), BF),
        vm((span_rows + 32, units), F32), vm((span_rows + 32, units), F32),
        vm((group, rows, width), BF), vm((group, half_rows, width), BF),
        vm((half_rows, width), F32), vm((group, half_rows, width), BF),
        vm((group, half_rows, width), BF), vm((half_rows, width), BF), vm((half_rows, width), BF),
        dma((6,)), dma((n,)), dma((n,)), dma((kv_heads,)), dma((kv_heads,)), *[dma((group,))] * 10,
        dma((kv_heads,)), dma((kv_heads,)), dma((2,)), dma((group,)), dma((group,)),
        dma((group,)), dma((group,)), dma((2 * group,)), dma((2 * group,)), dma((2,)),
        dma((group,)), dma((group,)),
        dma((group,)), dma((group,)), dma((2,)),
    ]
    args = (
        x_rows, queries, kv, query_norm_gain[None, :], key_norm_gain[None, :],
        cos, sin, out_weight, ffn_gain[None, :], *turned, taps[0], taps[1],
    )
    return pl.pallas_call(
        lambda *refs: layer_kernel(n, *refs),
        out_shape=jax.ShapeDtypeStruct((rows, width), BF),
        in_specs=[
            pl.BlockSpec(memory_space=pl.ANY if a is out_weight else pltpu.VMEM) for a in args
        ],
        out_specs=pl.BlockSpec(memory_space=pltpu.VMEM),
        scratch_shapes=scratch,
        compiler_params=pltpu.CompilerParams(
            collective_id=0, has_side_effects=True, vmem_limit_bytes=60 * 2**20
        ),
        name="layer",
    )(*args)


def suits(mesh, sizes):
    n, pair = mesh.shape["sp"], mesh.shape["tp"]
    x_rows, queries, keys, gate = sizes
    if pair != 2 or n % 4:
        return False
    rows, group = x_rows[0] // n, n // 2
    heads = keys[1] // pair // HEAD_SIZE
    units = gate[1] // pair
    return (
        rows % GRID_ROW_WIDTH == 0
        and rows % 32 == 0
        and queries[1] == 2 * keys[1]
        and n % heads == 0
        and 2 * HEAD_SIZE == LANES
        and x_rows[1] == n * LANES
        and units % (16 * group) == 0
    )


def solution(mesh):
    placed = (
        P("sp", None),
        P("sp", "tp"),
        P("sp", "tp"),
        P("sp", "tp"),
        P(),
        P(),
        P("tp", None),
        P(),
        P("sp", "tp"),
        P("sp", "tp"),
        P(None, "tp"),
        P(None, "tp"),
        P("sp", "tp"),
    )
    def run(*arrays):
        n = mesh.shape["sp"]
        fits = suits(mesh, [arrays[k].shape for k in (0, 1, 2, 8)])
        local = functools.partial(kernel_shards, n) if fits else shards
        return jax.shard_map(
            local, mesh=mesh, in_specs=placed, out_specs=P("sp", None), check_vma=False
        )(*arrays)

    return run
```
